32 devices in a mesh: fs: 16 (over z, y, x), tp: 2 (over core).
Axes of the slice: x: 2, y: 2, z: 4, core: 2. Of those that a mesh axis runs over, the one named last changes fastest.
Arguments:
- tokens: bfloat16 [12288, 2048], P('fs'), may hold values from -6 to 6
- norm_gain: float32 [2048], replicated, may hold values from 0.1 to 1.9
- up_weight: float32 [2048, 8192], P('fs', 'tp'), may hold values from -0.125 to 0.125
- up_scale: float32 [8192], P('tp'), may hold values from 0.5 to 2
- down_weight: float32 [8192, 2048], P('tp', 'fs'), may hold values from -0.09375 to 0.09375
- down_scale: float32 [1, 2048], replicated, may hold values from 0.5 to 2
Outputs:
- mixed: bfloat16 [12288, 2048], P('fs', 'tp')
The draws below stay inside these ranges and needn't reach their ends.
All inputs are finite; a program needn't handle non-finite values.
Results may differ from the reference program's by a relative error of at most 0.014.
Values may be sent and summed in bfloat16 or wider, within the bound.
A program may use at most 128 MiB of HBM per device.

```python
import math
import jax
import jax.numpy as jnp
from jax import lax

D = 2048
FF = 8192
TOKENS = 12288
N_FS = 16
N_TP = 2


def with_spikes(drawn, stream_key, source, target, shards_of, factor):
    def block_of(axis_at):
        return (jnp.arange(drawn.shape[axis_at]) // (drawn.shape[axis_at] // shards_of)).reshape((-1,) + (1,) * (drawn.ndim - 1 - axis_at))

    near = jax.random.permutation(stream_key, shards_of)[block_of(target)]
    far = (block_of(target) + shards_of // 2) % shards_of
    return jnp.where((block_of(source) == near) | (block_of(source) == far), factor * drawn, drawn)


def level_of(key, extent, cuts, low, high):
    level = 1.0
    for dim, shards_of in cuts:
        draws = jax.random.uniform(jax.random.fold_in(jax.random.fold_in(key, 6), dim), (shards_of,), jnp.float32, low / len(cuts), high / len(cuts))
        level = level * jnp.repeat(jnp.exp(draws), extent[dim] // shards_of).reshape((-1,) + (1,) * (len(extent) - 1 - dim))
    return level


def bell_draw(stream_key, extent, deviation, bound, shards=(), dtype=jnp.bfloat16):
    factor_of = level_of(stream_key, extent, shards, -0.22, 0.18) if shards else 1.0
    drawn = jax.random.normal(stream_key, extent, jnp.float32) * deviation * factor_of
    return jnp.minimum(jnp.maximum(drawn, -bound), bound).astype(dtype)


def gaussian_with(key, shape, spread, most, pieces, heavy, held_as=jnp.bfloat16):
    drawn = spread * jax.random.normal(key, shape, jnp.float32)
    if pieces:
        drawn = drawn * level_of(key, shape, pieces, -0.22, 0.18)
    return jnp.clip(with_spikes(drawn, jax.random.fold_in(key, 3), *heavy), -most, most).astype(held_as)


def setup_inputs(seed: int = 0) -> dict:
    arg_keys = jax.random.split(jax.random.key(seed), 7)
    tokens = bell_draw(arg_keys[0], (TOKENS, D), 1.0, 6.0, ((0, 16),))
    norm_gain = jnp.clip(1.0 + 0.18 * jax.random.normal(arg_keys[1], (D,), jnp.float32), 0.1, 1.9)
    up_weight = bell_draw(arg_keys[2], (D, FF), D ** -0.5, 0.125, ((0, 16), (1, 2)), jnp.float32)
    up_scale = jnp.clip(jnp.exp(math.log(2.0) - 1.3862944 * jax.random.uniform(arg_keys[3], (FF,), jnp.float32) ** level_of(arg_keys[3], (FF,), ((0, 2),), -0.2, 0.2)), 0.5, 2.0)
    down_weight = gaussian_with(arg_keys[4], (FF, D), FF ** -0.5, 0.09375, ((0, 2), (1, 16)), (0, 1, 16, 2.0), jnp.float32)
    down_scale = jnp.clip(jnp.exp(jax.random.uniform(arg_keys[5], (1, D), jnp.float32, math.log(0.5), math.log(2.0))), 0.5, 2.0)
    return dict(tokens=tokens, norm_gain=norm_gain, up_weight=up_weight, up_scale=up_scale, down_weight=down_weight, down_scale=down_scale)


def reference(tokens, norm_gain, up_weight, up_scale, down_weight, down_scale):
    up_cast = up_weight.astype(jnp.bfloat16)
    down_cast = down_weight.astype(jnp.bfloat16)
    block_ff = FF // N_TP
    groups = tokens.reshape(N_FS, TOKENS // N_FS, D)

    def one_group(rows):
        values = rows.astype(jnp.float32)
        normed = (values * lax.rsqrt(lax.optimization_barrier(jnp.mean(values * values, axis=-1, keepdims=True)) + 1e-06) * norm_gain).astype(jnp.bfloat16)
        pre = jnp.dot(normed, up_cast, preferred_element_type=jnp.float32) * up_scale
        hidden = jnp.square(jnp.maximum(pre, 0.0)).astype(jnp.bfloat16)
        total = jnp.zeros((rows.shape[0], D), jnp.float32)
        for block in range(N_TP):
            lower = block * block_ff
            partial_value = jnp.dot(hidden[:, lower:lower + block_ff], down_cast[lower:lower + block_ff, :], preferred_element_type=jnp.float32) * down_scale
            total = total + partial_value.astype(jnp.bfloat16).astype(jnp.float32)
        return total.astype(jnp.bfloat16)
    return lax.map(one_group, groups).reshape(TOKENS, D)
```

```python
import functools

import jax
import jax.numpy as jnp
from jax import lax
from jax.experimental import pallas as pl
from jax.experimental.pallas import tpu as pltpu
from jax.sharding import PartitionSpec as P

MESH = pl.DeviceIdType.MESH
SIDE = 2
GROUP = SIDE * SIDE
CORES = 2
COLS = 256
STRIP = 32


def gathered(tokens, norm_gain, up_weight, up_scale, down_weight, down_scale):
    values = tokens.astype(jnp.float32)
    normed = (
        values * lax.rsqrt(jnp.mean(values * values, axis=-1, keepdims=True) + 1e-06) * norm_gain
    ).astype(jnp.bfloat16)
    up_cast = up_weight.astype(jnp.bfloat16)
    down_cast = down_weight.astype(jnp.bfloat16)
    up_full = lax.all_gather(up_cast, "fs", axis=0, tiled=True)
    pre = jnp.dot(normed, up_full, preferred_element_type=jnp.float32) * up_scale
    hidden = jnp.square(jnp.maximum(pre, 0.0)).astype(jnp.bfloat16)
    down_full = lax.all_gather(down_cast, "fs", axis=1, tiled=True)
    partial_value = jnp.dot(hidden, down_full, preferred_element_type=jnp.float32) * down_scale
    rounded = partial_value.astype(jnp.bfloat16)
    return (
        lax.psum_scatter(rounded, "tp", scatter_dimension=1, tiled=True)
        .astype(jnp.float32)
        .astype(jnp.bfloat16)
    )


def layer_kernel(
    layers, rows, tokens, gain, up_in, down_in, up_scale, down_scale, out,
    tok, upb, downb, hid, stage, partner, summed, peers, own,
    up_wide, down_wide, up_cast, down_cast,
    local_sem, piece_recv, piece_send, level_send, tok_recv, tok_send,
    mate_recv, mate_send, part_recv, part_send, red_recv, red_send,
    end_part_recv, end_part_send, end_red_recv, end_red_send,
):
    fs = lax.axis_index("fs")
    core = lax.axis_index("tp")
    z, q = fs // GROUP, fs % GROUP
    depth, width = up_in.shape[0], upb.shape[1]
    half = rows // CORES
    sub = half // 2
    units = 2 * layers
    per_layer = GROUP * depth // COLS
    per_unit = COLS // depth

    def at(r):
        return ((q // SIDE + r // SIDE) % SIDE) * SIDE + (q % SIDE + r % SIDE) % SIDE

    def chip(layer, inner):
        return (layer * GROUP + inner, core)

    mate = (fs, 1 - core)

    barrier = pltpu.get_barrier_semaphore()
    for r in range(1, GROUP):
        pl.semaphore_signal(barrier, inc=1, device_id=chip(z, at(r)), device_id_type=MESH)
    pl.semaphore_signal(barrier, inc=1, device_id=mate, device_id_type=MESH)

    @pl.when(z > 0)
    def _():
        pl.semaphore_signal(barrier, inc=1, device_id=chip(z - 1, q), device_id_type=MESH)

    @pl.when(z < layers - 1)
    def _():
        pl.semaphore_signal(barrier, inc=1, device_id=chip(z + 1, q), device_id_type=MESH)

    def slot(kind, layer, inner):
        if kind == 0:
            return upb.at[pl.ds(pl.multiple_of((layer * GROUP + inner) * depth, depth), depth), :]
        return downb.at[layer, :, pl.ds(pl.multiple_of(inner * depth, depth), depth)]

    def source(kind, inner):
        return (up_cast if kind == 0 else down_cast).at[inner]

    def remote(src, dst, send, recv, device):
        return pltpu.make_async_remote_copy(
            src_ref=src, dst_ref=dst, send_sem=send, recv_sem=recv,
            device_id=device, device_id_type=MESH,
        )

    def along(kind, layer, inner, way):
        piece = slot(kind, layer, inner)
        index = layer * GROUP + inner
        return remote(
            piece, piece, piece_send.at[kind, index, way], piece_recv.at[kind, index],
            chip(z + 2 * way - 1, q),
        )

    def level(kind, r):
        return remote(
            source(kind, at(r)), slot(kind, z, q), level_send.at[kind, r - 1],
            piece_recv.at[kind, fs], chip(z, at(r)),
        )

    def each_way(kind, layer, inner, act):
        @pl.when(jnp.logical_and(layer <= z, z < layers - 1))
        def _():
            act(along(kind, layer, inner, 1))

        @pl.when(jnp.logical_and(layer >= z, z > 0))
        def _():
            act(along(kind, layer, inner, 0))

    def start(copy):
        copy.start()

    def finish_send(copy):
        copy.wait_send()

    def arrived(kind, layer, inner):
        piece = slot(kind, layer, inner)
        remote(
            piece, piece, piece_send.at[kind, layer * GROUP + inner, 0],
            piece_recv.at[kind, layer * GROUP + inner], mate,
        ).wait_recv()

    def block(inner, side, s):
        return tok.at[pl.ds(pl.multiple_of(inner * rows + side * half + s * sub, sub), sub), :]

    def hand(r, s):
        piece = block(q, core, s)
        return remote(piece, piece, tok_send.at[r - 1, s], tok_recv.at[r - 1, s], chip(z, at(r)))

    def pass_on(came, to, s):
        piece = block(at(came), core, s)
        return remote(
            piece, piece, tok_send.at[GROUP - 2, s], tok_recv.at[GROUP - 2, s], chip(z, at(to))
        )

    def tok_arrived(r, s):
        piece = block(at(r), core, s)
        remote(piece, piece, tok_send.at[r - 1, s], tok_recv.at[r - 1, s], mate).wait_recv()

    def share(r, s):
        piece = block(at(r), core, s)
        return remote(piece, piece, mate_send.at[r, s], mate_recv.at[r, s], mate)

    half_at = pl.ds(pl.multiple_of(q * rows + core * half, half), half)
    mine_at = pl.ds(pl.multiple_of(core * half, half), half)

    def wide(kind, r):
        part_at = pl.ds(pl.multiple_of(at(r) * width, width), width)
        if kind == 0:
            return pltpu.make_async_copy(up_in.at[:, part_at], up_wide.at[at(r)], local_sem.at[0, r])
        return pltpu.make_async_copy(down_in.at[part_at, :], down_wide.at[at(r)], local_sem.at[1, r])

    token_copy = pltpu.make_async_copy(tokens.at[mine_at, :], tok.at[half_at, :], local_sem.at[2, 0])
    for r in range(GROUP):
        wide(0, r).start()
    token_copy.start()
    for r in range(GROUP):
        wide(1, r).start()
    wide(0, 0).wait()
    upb[pl.ds(pl.multiple_of(fs * depth, depth), depth), :] = up_wide[q].astype(upb.dtype)
    for r in range(1, GROUP):
        wide(0, r).wait()
        up_cast[at(r)] = up_wide[at(r)].astype(up_cast.dtype)

    greeted = GROUP + jnp.where(z > 0, 1, 0) + jnp.where(z < layers - 1, 1, 0)
    pl.semaphore_wait(barrier, greeted)

    each_way(0, z, q, start)
    for r in (1, 2, 3):
        level(0, r).start()

    def normalize(i, carry):
        strip = pl.ds(pl.multiple_of(q * rows + core * half + i * STRIP, STRIP), STRIP)
        values = tok[strip, :].astype(jnp.float32)
        mean = jnp.mean(values * values, axis=-1, keepdims=True)
        tok[strip, :] = (values * lax.rsqrt(mean + 1e-06) * gain[...]).astype(tok.dtype)
        return carry

    token_copy.wait()
    lax.fori_loop(0, half // STRIP, normalize, 0)
    hand(1, 0).start()
    hand(2, 1).start()
    hand(1, 1).start()
    hand(2, 0).start()
    wide(1, 0).wait()
    downb[z, :, pl.ds(pl.multiple_of(q * depth, depth), depth)] = down_wide[q].astype(downb.dtype)
    for r in range(1, GROUP):
        wide(1, r).wait()
        down_cast[at(r)] = down_wide[at(r)].astype(down_cast.dtype)
    for r in (1, 2, 3):
        level(1, r).start()
    for s in (0, 1):
        share(0, s).start()

    inside = jnp.logical_and(z > 0, z < layers - 1)

    def near(r):
        arrived(0, z, at(r))
        each_way(0, z, at(r), start)

    def afar(d, r):
        for layer, there in ((z - d, z - d >= 0), (z + d, z + d < layers)):
            @pl.when(there)
            def _():
                arrived(0, layer, at(r))
                each_way(0, layer, at(r), start)

    def when_inside(d, rs):
        @pl.when(inside)
        def _():
            for r in rs:
                afar(d, r)

    near(1)
    near(2)
    when_inside(1, (0,))
    near(3)
    when_inside(1, (1, 2, 3))
    tok_arrived(1, 0)
    pass_on(1, 2, 0).start()
    share(1, 0).start()
    tok_arrived(2, 1)
    pass_on(2, 1, 1).start()
    share(2, 1).start()
    for d in range(2, layers):
        when_inside(d, range(GROUP))
    for r, s in ((1, 1), (2, 0)):
        tok_arrived(r, s)
        share(r, s).start()
    for r in (1, 2, 3):
        arrived(1, z, at(r))
    for i in range(GROUP):
        each_way(1, z, i, start)

    @pl.when(jnp.logical_not(inside))
    def _():
        for d in range(1, layers):
            for r in range(GROUP):
                afar(d, r)

    def take(d, r):
        for layer, there in ((z - d, z - d >= 0), (z + d, z + d < layers)):
            @pl.when(there)
            def _():
                arrived(1, layer, r)
                each_way(1, layer, r, start)

    wide_n = COLS
    across = width // wide_n
    turn = jnp.where(inside, GROUP - 1, GROUP - 2)

    def first(i, carry):
        r = i // across
        b = at(r)

        @pl.when(i == turn * across)
        def _():
            for s in (0, 1):
                tok_arrived(3, s)
                share(3, s).start()

        @pl.when(i % across == 0)
        def _():
            for s in (0, 1):
                piece = block(b, 1 - core, s)
                remote(piece, piece, mate_send.at[r, s], mate_recv.at[r, s], mate).wait_recv()

        m = pl.ds(pl.multiple_of(b * rows, rows), rows)
        at_n = pl.multiple_of((i % across) * wide_n, wide_n)
        pre = jnp.dot(tok[m, :], upb[:, pl.ds(at_n, wide_n)], preferred_element_type=jnp.float32)
        pre = pre * up_scale[:, pl.ds(pl.multiple_of(q * width + at_n, wide_n), wide_n)]
        hid[m, pl.ds(at_n, wide_n)] = jnp.square(jnp.maximum(pre, 0.0)).astype(hid.dtype)
        return carry

    lax.fori_loop(0, GROUP * across, first, 0)

    @pl.when(inside)
    def _():
        for r in range(GROUP):
            take(1, r)

    upper, lower = pl.ds(0, half), pl.ds(half, half)
    hops = ((3, upper, 2, 1), (3, lower, 2, 2), (1, upper, 0, 1), (2, lower, 1, 2),
            (1, lower, 0, 1), (2, upper, 1, 2))

    def red(u, k):
        of, part_rows, into, to = hops[k]
        return remote(
            summed.at[u, at(of), part_rows, :], peers.at[u, into, part_rows, :],
            red_send.at[u, k], red_recv.at[u, k], chip(z, at(to)),
        )

    def relay(u):
        for k, of, part_rows, then in ((0, 2, upper, 5), (1, 1, lower, 4)):
            red(u, k).wait_recv()
            total = summed[u, at(of), part_rows, :].astype(jnp.float32)
            total = total + peers[u, 2, part_rows, :].astype(jnp.float32)
            summed[u, at(of), part_rows, :] = total.astype(summed.dtype)
            red(u, then).start()

    def unit_of(t):
        s, h = t // per_layer, t % per_layer
        layer = jnp.where(
            2 * z < layers,
            jnp.where(s <= z, z - s, s),
            jnp.where(s <= layers - 1 - z, z + s, layers - 1 - s),
        )
        unit = layer * per_layer + h
        return s, h, layer, unit, unit // (units // CORES), unit % (units // CORES)

    def part(u, b):
        return remote(
            stage.at[u, b], partner.at[u, b], part_send.at[u, b], part_recv.at[u, b], mate
        )

    def second(t, carry):
        s, h, layer, unit, owner, u = unit_of(t)

        @pl.when(s > jnp.where(inside, 1, 0))
        def _():
            for k in range(per_unit):
                take(s, h * per_unit + k)

        cols = pl.ds(pl.multiple_of(h * COLS, COLS), COLS)
        scale = pl.ds(pl.multiple_of(unit * COLS, COLS), COLS)

        def product(b):
            m = pl.ds(pl.multiple_of(b * rows, rows), rows)
            value = jnp.dot(hid[m, :], downb[layer, :, cols], preferred_element_type=jnp.float32)
            return value * down_scale[:, scale]

        @pl.when(owner != core)
        def _():
            def away(i, c):
                b = at(GROUP - 1 - i)
                stage[u, b] = product(b).astype(stage.dtype)
                part(u, b).start()
                return c

            lax.fori_loop(0, GROUP, away, 0)

        @pl.when(owner == core)
        def _():
            def mine(i, c):
                own[at(GROUP - 1 - i)] = product(at(GROUP - 1 - i))
                return c

            lax.fori_loop(0, GROUP, mine, 0)
            for r in (3, 2, 1, 0):
                b = at(r)
                part(u, b).wait_recv()
                summed[u, b] = (own[b] + partner[u, b].astype(jnp.float32)).astype(summed.dtype)
                for k in {3: (0, 1), 1: (2,), 2: (3,), 0: ()}[r]:
                    red(u, k).start()

        before = unit_of(jnp.maximum(t - 1, 0))

        @pl.when(jnp.logical_and(t > 0, before[4] == core))
        def _():
            relay(before[5])

        return carry

    lax.fori_loop(0, units - 1, second, 0)
    before = unit_of(units - 2)

    @pl.when(before[4] == core)
    def _():
        relay(before[5])

    s_end, h_end, layer_end, unit_end, owner_end, u_end = unit_of(units - 1)
    mine_end = owner_end == core
    thin = COLS // 2

    def end_part(e, r):
        piece = pl.ds(e * thin, thin)
        return remote(
            stage.at[u_end, at(r), :, piece], partner.at[u_end, at(r), :, piece],
            end_part_send.at[e, r], end_part_recv.at[e, r], mate,
        )

    def end_red(e, r):
        piece = pl.ds(e * thin, thin)
        return remote(
            summed.at[u_end, at(r), :, piece], peers.at[u_end, r - 1, :, piece],
            end_red_send.at[e, r - 1], end_red_recv.at[e, r - 1], chip(z, at(r)),
        )

    for e in range(2):
        @pl.when(s_end > jnp.where(inside, 1, 0))
        def _():
            for k in ((e,) if per_unit == 2 else range(per_unit * (1 - e))):
                take(s_end, h_end * per_unit + k)

        piece = pl.ds(e * thin, thin)
        cols = pl.ds(pl.multiple_of(h_end * COLS + e * thin, thin), thin)
        scale = pl.ds(pl.multiple_of(unit_end * COLS + e * thin, thin), thin)

        def product(r):
            m = pl.ds(pl.multiple_of(at(r) * rows, rows), rows)
            value = jnp.dot(
                hid[m, :], downb[layer_end, :, cols], preferred_element_type=jnp.float32
            )
            return value * down_scale[:, scale]

        @pl.when(jnp.logical_not(mine_end))
        def _():
            for r in (3, 1, 2, 0):
                stage[u_end, at(r), :, piece] = product(r).astype(stage.dtype)
                end_part(e, r).start()

        @pl.when(mine_end)
        def _():
            def gather(r):
                end_part(e, r).wait_recv()
                total = own[r, :, piece] + partner[u_end, at(r), :, piece].astype(jnp.float32)
                summed[u_end, at(r), :, piece] = total.astype(summed.dtype)
                if r:
                    end_red(e, r).start()

            order = (3, 1, 2, 0)
            for i, r in enumerate(order):
                own[r, :, piece] = product(r)
                if i > 1:
                    gather(order[i - 2])
            gather(order[2])
            gather(order[3])

    def last(u, carry):
        @pl.when(jnp.logical_not(jnp.logical_and(mine_end, u == u_end)))
        def _():
            for k in range(2, 6):
                red(u, k).wait_recv()
            total = summed[u, q].astype(jnp.float32)
            for side in range(2):
                total = total + peers[u, side].astype(jnp.float32)
            out[:, pl.ds(pl.multiple_of(u * COLS, COLS), COLS)] = total.astype(out.dtype)

        return carry

    lax.fori_loop(0, units // CORES, last, 0)

    @pl.when(mine_end)
    def _():
        for e in range(2):
            piece = pl.ds(e * thin, thin)
            for r in (1, 2, 3):
                end_red(e, r).wait_recv()
            total = summed[u_end, q, :, piece].astype(jnp.float32)
            for side in range(3):
                total = total + peers[u_end, side, :, piece].astype(jnp.float32)
            to = pl.ds(pl.multiple_of(u_end * COLS + e * thin, thin), thin)
            out[:, to] = total.astype(out.dtype)

    def drain(u, carry):
        @pl.when(jnp.logical_not(jnp.logical_and(mine_end, u == u_end)))
        def _():
            for k in range(len(hops)):
                red(u, k).wait_send()

        @pl.when(jnp.logical_or(mine_end, u != u_end))
        def _():
            for b in range(GROUP):
                part(u, b).wait_send()

        return carry

    lax.fori_loop(0, units // CORES, drain, 0)

    @pl.when(mine_end)
    def _():
        for e in range(2):
            for r in (1, 2, 3):
                end_red(e, r).wait_send()

    @pl.when(jnp.logical_not(mine_end))
    def _():
        for e in range(2):
            for r in range(GROUP):
                end_part(e, r).wait_send()

    for kind in (0, 1):
        for r in range(1, GROUP):
            level(kind, r).wait_send()

        def drained(i, carry):
            each_way(kind, i // GROUP, i % GROUP, finish_send)
            return carry

        lax.fori_loop(0, layers * GROUP, drained, 0)
    for r in (1, 2):
        for s in (0, 1):
            hand(r, s).wait_send()
    pass_on(1, 2, 0).wait_send()
    pass_on(2, 1, 1).wait_send()
    for r in (0, 1, 2, 3):
        for s in (0, 1):
            share(r, s).wait_send()


def grouped(layers, tokens, norm_gain, up_weight, up_scale, down_weight, down_scale):
    rows, model = tokens.shape
    depth = up_weight.shape[0]
    width = up_weight.shape[1] // GROUP
    share = model // COLS // CORES
    n = layers * GROUP
    dma = pltpu.SemaphoreType.DMA
    vmem = pl.BlockSpec(memory_space=pltpu.VMEM)
    hbm = pl.BlockSpec(memory_space=pltpu.HBM)
    return pl.pallas_call(
        functools.partial(layer_kernel, layers, rows),
        out_shape=pltpu.VMEM((rows, model // CORES), jnp.bfloat16),
        in_specs=[hbm, vmem, hbm, hbm, vmem, vmem],
        out_specs=vmem,
        scratch_shapes=[
            pltpu.VMEM((GROUP * rows, model), jnp.bfloat16),
            pltpu.VMEM((model, width), jnp.bfloat16),
            pltpu.VMEM((layers, width, GROUP * depth), jnp.bfloat16),
            pltpu.VMEM((GROUP * rows, width), jnp.bfloat16),
            pltpu.VMEM((share, GROUP, rows, COLS), jnp.bfloat16),
            pltpu.VMEM((share, GROUP, rows, COLS), jnp.bfloat16),
            pltpu.VMEM((share, GROUP, rows, COLS), jnp.bfloat16),
            pltpu.VMEM((share, GROUP - 1, rows, COLS), jnp.bfloat16),
            pltpu.VMEM((GROUP, rows, COLS), jnp.float32),
            pltpu.VMEM((GROUP, depth, width), jnp.float32),
            pltpu.VMEM((GROUP, width, depth), jnp.float32),
            pltpu.VMEM((GROUP, depth, width), jnp.bfloat16),
            pltpu.VMEM((GROUP, width, depth), jnp.bfloat16),
            dma((3, GROUP)),
            dma((2, n)),
            dma((2, n, 2)),
            dma((2, GROUP - 1)),
            dma((GROUP - 1, 2)),
            dma((GROUP - 1, 2)),
            dma((GROUP, 2)),
            dma((GROUP, 2)),
            dma((share, GROUP)),
            dma((share, GROUP)),
            dma((share, 6)),
            dma((share, 6)),
            dma((2, GROUP)),
            dma((2, GROUP)),
            dma((2, GROUP - 1)),
            dma((2, GROUP - 1)),
        ],
        compiler_params=pltpu.CompilerParams(
            collective_id=0, has_side_effects=True, vmem_limit_bytes=60 * 2**20
        ),
    )(
        tokens, norm_gain.reshape(1, -1), up_weight, down_weight, up_scale.reshape(1, -1), down_scale
    )


def solution(mesh):
    fs, tp = mesh.shape["fs"], mesh.shape["tp"]
    if tp == CORES and fs % (2 * GROUP) == 0 and fs <= 4 * GROUP:
        body = functools.partial(grouped, fs // GROUP)
    else:
        body = gathered
    in_specs = (P("fs", None), P(), P("fs", "tp"), P("tp"), P("tp", "fs"), P())
    out_specs = P("fs", "tp")
    return jax.shard_map(
        body, mesh=mesh, in_specs=in_specs, out_specs=out_specs, check_vma=False
    )
```

```python
import functools

import jax
import jax.numpy as jnp
from jax import lax
from jax.experimental import pallas as pl
from jax.experimental.pallas import tpu as pltpu
from jax.sharding import PartitionSpec as P

MESH = pl.DeviceIdType.MESH
SIDE = 2
GROUP = SIDE * SIDE
CORES = 2
COLS = 256
STRIP = 32


def gathered(tokens, norm_gain, up_weight, up_scale, down_weight, down_scale):
    values = tokens.astype(jnp.float32)
    normed = (
        values * lax.rsqrt(jnp.mean(values * values, axis=-1, keepdims=True) + 1e-06) * norm_gain
    ).astype(jnp.bfloat16)
    up_cast = up_weight.astype(jnp.bfloat16)
    down_cast = down_weight.astype(jnp.bfloat16)
    up_full = lax.all_gather(up_cast, "fs", axis=0, tiled=True)
    pre = jnp.dot(normed, up_full, preferred_element_type=jnp.float32) * up_scale
    hidden = jnp.square(jnp.maximum(pre, 0.0)).astype(jnp.bfloat16)
    down_full = lax.all_gather(down_cast, "fs", axis=1, tiled=True)
    partial_value = jnp.dot(hidden, down_full, preferred_element_type=jnp.float32) * down_scale
    rounded = partial_value.astype(jnp.bfloat16)
    return (
        lax.psum_scatter(rounded, "tp", scatter_dimension=1, tiled=True)
        .astype(jnp.float32)
        .astype(jnp.bfloat16)
    )


def layer_kernel(
    layers, rows, tokens, gain_in, up_in, down_in, up_scale_in, down_scale_in, out,
    gain, up_scale, down_scale, tok, upb, downb, hid, stage, partner, summed, peers, own,
    up_wide, down_wide, up_cast, down_cast,
    local_sem, piece_recv, piece_send, level_send, near_recv, tok_recv, mate_recv,
    part_recv, red_recv, end_red_recv, sent,
):
    fs = lax.axis_index("fs")
    core = lax.axis_index("tp")
    z, q = fs // GROUP, fs % GROUP
    depth, width = up_in.shape[0], upb.shape[1]
    half = rows // CORES
    sub = half // 2
    units = 2 * layers
    per_layer = GROUP * depth // COLS
    per_unit = COLS // depth

    def at(r):
        return ((q // SIDE + r // SIDE) % SIDE) * SIDE + (q % SIDE + r % SIDE) % SIDE

    def chip(layer, inner):
        return (layer * GROUP + inner, core)

    mate = (fs, 1 - core)

    barrier = pltpu.get_barrier_semaphore()
    for r in range(1, GROUP):
        pl.semaphore_signal(barrier, inc=1, device_id=chip(z, at(r)), device_id_type=MESH)
    pl.semaphore_signal(barrier, inc=1, device_id=mate, device_id_type=MESH)

    @pl.when(z > 0)
    def _():
        pl.semaphore_signal(barrier, inc=1, device_id=chip(z - 1, q), device_id_type=MESH)

    @pl.when(z < layers - 1)
    def _():
        pl.semaphore_signal(barrier, inc=1, device_id=chip(z + 1, q), device_id_type=MESH)

    def slot(kind, layer, inner):
        if kind == 0:
            return upb.at[pl.ds(pl.multiple_of((layer * GROUP + inner) * depth, depth), depth), :]
        return downb.at[layer, :, pl.ds(pl.multiple_of(inner * depth, depth), depth)]

    tok_send, mate_send, part_send, red_send = (sent.at[i] for i in range(4))

    def source(kind, inner):
        return (up_cast if kind == 0 else down_cast).at[inner]

    def remote(src, dst, send, recv, device):
        return pltpu.make_async_remote_copy(
            src_ref=src, dst_ref=dst, send_sem=send, recv_sem=recv,
            device_id=device, device_id_type=MESH,
        )

    def along(kind, layer, inner, way):
        piece = slot(kind, layer, inner)
        index = layer * GROUP + inner
        return remote(
            piece, piece, piece_send.at[kind, way], piece_recv.at[kind, index],
            chip(z + 2 * way - 1, q),
        )

    def level(r):
        return remote(
            source(1, at(r)), slot(1, z, q), level_send.at[1],
            piece_recv.at[1, fs], chip(z, at(r)),
        )

    def first_rows(h, inner=q):
        lower = (z * GROUP + inner) * depth + h * (depth // 2)
        return upb.at[pl.ds(pl.multiple_of(lower, depth // 2), depth // 2), :]

    def near_half(r, h):
        return remote(
            source(0, at(r)).at[pl.ds(h * (depth // 2), depth // 2), :], first_rows(h),
            level_send.at[0], near_recv.at[r - 1, h], chip(z, at(r)),
        )

    def half_along(inner, way, h):
        piece = first_rows(h, inner)
        index = z * GROUP + inner
        return remote(
            piece, piece, piece_send.at[0, way], piece_recv.at[0, index],
            chip(z + 2 * way - 1, q),
        )

    def each_way(kind, layer, inner, act):
        @pl.when(jnp.logical_and(layer <= z, z < layers - 1))
        def _():
            act(along(kind, layer, inner, 1))

        @pl.when(jnp.logical_and(layer >= z, z > 0))
        def _():
            act(along(kind, layer, inner, 0))

    def start(copy):
        copy.start()

    def finish_send(copy):
        copy.wait_send()

    def arrived(kind, layer, inner):
        piece = slot(kind, layer, inner)
        remote(
            piece, piece, piece_send.at[kind, 0],
            piece_recv.at[kind, layer * GROUP + inner], mate,
        ).wait_recv()

    def block(inner, side, s):
        return tok.at[pl.ds(pl.multiple_of(inner * rows + side * half + s * sub, sub), sub), :]

    def hand(r, s):
        piece = block(q, core, s)
        return remote(piece, piece, tok_send, tok_recv.at[r - 1, s], chip(z, at(r)))

    def pass_on(came, to, s):
        piece = block(at(came), core, s)
        return remote(
            piece, piece, tok_send, tok_recv.at[GROUP - 2, s], chip(z, at(to))
        )

    def tok_arrived(r, s):
        piece = block(at(r), core, s)
        remote(piece, piece, tok_send, tok_recv.at[r - 1, s], mate).wait_recv()

    def share(r, s):
        piece = block(at(r), core, s)
        return remote(piece, piece, mate_send, mate_recv.at[r], mate)

    half_at = pl.ds(pl.multiple_of(q * rows + core * half, half), half)
    mine_at = pl.ds(pl.multiple_of(core * half, half), half)

    down_copy = pltpu.make_async_copy(down_in, down_wide, local_sem.at[1])
    token_copy = pltpu.make_async_copy(tokens.at[mine_at, :], tok.at[half_at, :], local_sem.at[2])
    small = [
        pltpu.make_async_copy(gain_in, gain, local_sem.at[3]),
        pltpu.make_async_copy(up_scale_in, up_scale, local_sem.at[4]),
        pltpu.make_async_copy(down_scale_in, down_scale, local_sem.at[5]),
    ]

    def part_at(r):
        return pl.ds(pl.multiple_of(at(r) * width, width), width)

    def up_copy(r):
        return pltpu.make_async_copy(
            up_in.at[:, part_at(r)], up_wide.at[:, part_at(r)], local_sem.at[6 if r else 0]
        )

    for r in range(GROUP):
        up_copy(r).start()
    token_copy.start()
    for copy in small:
        copy.start()
    down_copy.start()
    up_copy(0).wait()
    own_rows = pl.ds(pl.multiple_of(fs * depth, depth), depth)
    upb[own_rows, :] = up_wide[:, part_at(0)].astype(upb.dtype)
    greeted = GROUP + jnp.where(z > 0, 1, 0) + jnp.where(z < layers - 1, 1, 0)
    pl.semaphore_wait(barrier, greeted)
    each_way(0, z, q, start)
    others = up_wide.at[:, pl.ds(0, (GROUP - 1) * width)]
    pltpu.make_async_copy(others, others, local_sem.at[6]).wait()
    for r in range(1, GROUP):
        up_cast[at(r)] = up_wide[:, part_at(r)].astype(up_cast.dtype)

    for r in (1, 2, 3):
        for h in (0, 1):
            near_half(r, h).start()

    def normalize(i, carry):
        strip = pl.ds(pl.multiple_of(q * rows + core * half + i * STRIP, STRIP), STRIP)
        values = tok[strip, :].astype(jnp.float32)
        mean = jnp.mean(values * values, axis=-1, keepdims=True)
        tok[strip, :] = (values * lax.rsqrt(mean + 1e-06) * gain[...]).astype(tok.dtype)
        return carry

    token_copy.wait()
    small[0].wait()
    lax.fori_loop(0, half // STRIP, normalize, 0)

    hand(1, 0).start()
    hand(2, 1).start()
    hand(1, 1).start()
    hand(2, 0).start()
    down_copy.wait()
    own_cols = pl.ds(pl.multiple_of(q * depth, depth), depth)
    downb[z, :, own_cols] = down_wide[part_at(0), :].astype(downb.dtype)
    for r in range(1, GROUP):
        down_cast[at(r)] = down_wide[part_at(r), :].astype(down_cast.dtype)
    for r in (1, 2, 3):
        level(r).start()
    for s in (0, 1):
        share(0, s).start()

    inside = jnp.logical_and(z > 0, z < layers - 1)

    def near(r, h):
        piece = first_rows(h, at(r))
        remote(piece, piece, level_send.at[0], near_recv.at[r - 1, h], mate).wait_recv()

        @pl.when(z < layers - 1)
        def _():
            half_along(at(r), 1, h).start()

        @pl.when(z > 0)
        def _():
            half_along(at(r), 0, h).start()

    def afar(d, r):
        for layer, there in ((z - d, z - d >= 0), (z + d, z + d < layers)):
            @pl.when(there)
            def _():
                arrived(0, layer, at(r))
                each_way(0, layer, at(r), start)

    def when_inside(d, rs):
        @pl.when(inside)
        def _():
            for r in rs:
                afar(d, r)

    for h in (0, 1):
        for r in (1, 2):
            near(r, h)
    when_inside(1, (0,))
    for h in (0, 1):
        near(3, h)
    when_inside(1, (1, 2, 3))
    tok_arrived(1, 0)
    pass_on(1, 2, 0).start()
    share(1, 0).start()
    tok_arrived(2, 1)
    pass_on(2, 1, 1).start()
    share(2, 1).start()
    for d in range(2, layers):
        when_inside(d, range(GROUP))
    for r, s in ((1, 1), (2, 0)):
        tok_arrived(r, s)
        share(r, s).start()
    for r in (1, 2, 3):
        arrived(1, z, at(r))
    for i in range(GROUP):
        each_way(1, z, i, start)

    @pl.when(jnp.logical_not(inside))
    def _():
        for d in range(1, layers):
            for r in range(GROUP):
                afar(d, r)

    def take(d, r):
        for layer, there in ((z - d, z - d >= 0), (z + d, z + d < layers)):
            @pl.when(there)
            def _():
                arrived(1, layer, r)
                each_way(1, layer, r, start)

    wide_n = COLS
    across = width // wide_n
    turn = jnp.where(inside, GROUP - 1, GROUP - 2)

    def first(i, carry):
        r = i // across
        b = at(r)

        @pl.when(i == turn * across)
        def _():
            for s in (0, 1):
                tok_arrived(3, s)
                share(3, s).start()

        @pl.when(i % across == 0)
        def _():
            theirs = pl.ds(pl.multiple_of(b * rows + (1 - core) * half, half), half)
            piece = tok.at[theirs, :]
            remote(piece, piece, mate_send, mate_recv.at[r], mate).wait_recv()

        m = pl.ds(pl.multiple_of(b * rows, rows), rows)
        at_n = pl.multiple_of((i % across) * wide_n, wide_n)
        pre = jnp.dot(tok[m, :], upb[:, pl.ds(at_n, wide_n)], preferred_element_type=jnp.float32)
        pre = pre * up_scale[:, pl.ds(pl.multiple_of(q * width + at_n, wide_n), wide_n)]
        hid[m, pl.ds(at_n, wide_n)] = jnp.square(jnp.maximum(pre, 0.0)).astype(hid.dtype)
        return carry

    small[1].wait()
    small[2].wait()
    lax.fori_loop(0, GROUP * across, first, 0)

    @pl.when(inside)
    def _():
        for r in range(GROUP):
            take(1, r)

    upper, lower = pl.ds(0, half), pl.ds(half, half)
    hops = ((3, upper, 2, 1), (3, lower, 2, 2), (1, upper, 0, 1), (2, lower, 1, 2),
            (1, lower, 0, 1), (2, upper, 1, 2))

    def red(u, k):
        of, part_rows, into, to = hops[k]
        return remote(
            summed.at[u, at(of), :, part_rows, :], peers.at[u, into, :, part_rows, :],
            red_send, red_recv.at[u, min(k, 2)], chip(z, at(to)),
        )

    relays = ((0, 2, upper, 5), (1, 1, lower, 4))

    def relay(u):
        for k, of, part_rows, then in relays:
            red(u, k).wait_recv()
            total = summed[u, at(of), :, part_rows, :].astype(jnp.float32)
            total = total + peers[u, 2, :, part_rows, :].astype(jnp.float32)
            summed[u, at(of), :, part_rows, :] = total.astype(summed.dtype)
            red(u, then).start()

    def unit_of(t):
        s, h = t // per_layer, t % per_layer
        layer = jnp.where(
            2 * z < layers,
            jnp.where(s <= z, z - s, s),
            jnp.where(s <= layers - 1 - z, z + s, layers - 1 - s),
        )
        unit = layer * per_layer + h
        return s, h, layer, unit, unit // (units // CORES), unit % (units // CORES)

    def part(u, b):
        return remote(
            stage.at[u, b], partner.at[u, b], part_send, part_recv.at[u, b], mate
        )

    thin = COLS // 2

    def second(t, carry):
        s, h, layer, unit, owner, u = unit_of(t)

        @pl.when(s > jnp.where(inside, 1, 0))
        def _():
            for k in range(per_unit):
                take(s, h * per_unit + k)

        cols = pl.ds(pl.multiple_of(h * COLS, COLS), COLS)
        scale = pl.ds(pl.multiple_of(unit * COLS, COLS), COLS)

        def product(b):
            m = pl.ds(pl.multiple_of(b * rows, rows), rows)
            value = jnp.dot(hid[m, :], downb[layer, :, cols], preferred_element_type=jnp.float32)
            return value * down_scale[:, scale]

        @pl.when(owner != core)
        def _():
            def away(i, c):
                b = at(GROUP - 1 - i)
                value = product(b).astype(stage.dtype)
                for e in range(2):
                    stage[u, b, e] = value[:, e * thin:(e + 1) * thin]
                part(u, b).start()
                return c

            lax.fori_loop(0, GROUP, away, 0)

        @pl.when(owner == core)
        def _():
            def mine(i, c):
                own[at(GROUP - 1 - i)] = product(at(GROUP - 1 - i))
                return c

            lax.fori_loop(0, GROUP, mine, 0)
            for r in (3, 2, 1, 0):
                b = at(r)
                part(u, b).wait_recv()
                for e in range(2):
                    total = own[b, :, e * thin:(e + 1) * thin]
                    total = total + partner[u, b, e].astype(jnp.float32)
                    summed[u, b, e] = total.astype(summed.dtype)
                for k in {3: (0, 1), 1: (2,), 2: (3,), 0: ()}[r]:
                    red(u, k).start()

        before = unit_of(jnp.maximum(t - 1, 0))

        @pl.when(jnp.logical_and(t > 0, before[4] == core))
        def _():
            relay(before[5])

        return carry

    tail = units - per_layer
    lax.fori_loop(0, tail, second, 0)
    before = unit_of(tail - 1)
    mine_end = unit_of(tail)[4] == core

    @pl.when(jnp.logical_and(before[4] == core, jnp.logical_not(mine_end)))
    def _():
        relay(before[5])

    def end_part(u, e, r):
        return remote(
            stage.at[u, at(r), e], partner.at[u, at(r), e],
            part_send, part_recv.at[u, 2 * e + (0 if r == 3 else 1)], mate,
        )

    def end_rows(k, i):
        base = hops[k][1].start
        return pl.ds(base, half) if i is None else pl.ds(base + i * sub, sub)

    def end_red(u, e, k, i=None):
        of, _, into, to = hops[k]
        come = 2 * k + i if k < 2 else 4
        return remote(
            summed.at[u, at(of), e, end_rows(k, i), :], peers.at[u, into, e, end_rows(k, i), :],
            red_send, end_red_recv.at[u % per_layer, e, come], chip(z, at(to)),
        )

    def end_relay(u, e):
        for i in range(2):
            for k, of, _, then in relays:
                end_red(u, e, k, i).wait_recv()
                total = summed[u, at(of), e, end_rows(k, i), :].astype(jnp.float32)
                total = total + peers[u, 2, e, end_rows(k, i), :].astype(jnp.float32)
                summed[u, at(of), e, end_rows(k, i), :] = total.astype(summed.dtype)
                end_red(u, e, then, i).start()

    def ending(v, carry):
        e = v % 2
        s, h, layer, unit, owner, u = unit_of(tail + v // 2)

        @pl.when(s > jnp.where(inside, 1, 0))
        def _():
            take(s, h * per_unit + e)

        cols = pl.ds(pl.multiple_of(h * COLS + e * thin, thin), thin)
        scale = pl.ds(pl.multiple_of(unit * COLS + e * thin, thin), thin)

        def product(r, into):
            for i in range(CORES):
                m = pl.ds(pl.multiple_of(at(r) * rows + i * half, half), half)
                value = jnp.dot(
                    hid[m, :], downb[layer, :, cols], preferred_element_type=jnp.float32
                )
                value = value * down_scale[:, scale]
                into[pl.ds(i * half, half), :] = value.astype(into.dtype)

        @pl.when(jnp.logical_not(mine_end))
        def _():
            for r in (3, 1, 2, 0):
                product(r, stage.at[u, at(r), e])
                end_part(u, e, r).start()

        @pl.when(mine_end)
        def _():
            def compute(r):
                product(r, own.at[r, :, pl.ds(0, thin)])

            def gather(r):
                if r == 3:
                    end_part(u, e, r).wait_recv()
                elif r == 1:
                    rest = partner.at[u, pl.ds(0, GROUP - 1), e]
                    remote(rest, rest, part_send, part_recv.at[u, 2 * e + 1], mate).wait_recv()
                total = own[r, :, :thin] + partner[u, at(r), e].astype(jnp.float32)
                summed[u, at(r), e] = total.astype(summed.dtype)
                if r == 3:
                    for i in range(2):
                        for k in range(2):
                            end_red(u, e, k, i).start()
                elif r:
                    end_red(u, e, r + 1).start()

            compute(3)
            gather(3)

            @pl.when(jnp.logical_and(v == 0, before[4] == core))
            def _():
                relay(before[5])

            @pl.when(v > 0)
            def _():
                end_relay(unit_of(tail + (v - 1) // 2)[5], (v - 1) % 2)

            compute(1)
            compute(2)
            gather(1)
            compute(0)
            gather(2)
            gather(0)

        return carry

    lax.fori_loop(0, 2 * per_layer, ending, 0)

    @pl.when(mine_end)
    def _():
        end_relay(unit_of(units - 1)[5], 1)

    def last(t, carry):
        owner, u = unit_of(t)[4:]

        @pl.when(owner == core)
        def _():
            arrive = peers.at[u, pl.ds(0, 2)]
            remote(arrive, arrive, red_send, red_recv.at[u, 2], mate).wait_recv()
            for e in range(2):
                total = summed[u, q, e].astype(jnp.float32)
                for side in range(2):
                    total = total + peers[u, side, e].astype(jnp.float32)
                at_e = pl.ds(pl.multiple_of(u * COLS + e * thin, thin), thin)
                out[:, at_e] = total.astype(out.dtype)

        return carry

    lax.fori_loop(0, tail, last, 0)

    def finish(v, carry):
        e = v % 2
        u = unit_of(tail + v // 2)[5]
        arrive = peers.at[u, pl.ds(0, 2), e]
        remote(arrive, arrive, red_send, end_red_recv.at[u % per_layer, e, 4], mate).wait_recv()
        total = summed[u, q, e].astype(jnp.float32)
        for side in range(2):
            total = total + peers[u, side, e].astype(jnp.float32)
        at_e = pl.ds(pl.multiple_of(u * COLS + e * thin, thin), thin)
        out[:, at_e] = total.astype(out.dtype)
        return carry

    def wait_sent(piece, send):
        remote(piece, piece, send, piece_recv.at[0, 0], mate).wait_send()

    def drain_early():
        for kind in (0, 1):
            wait_sent(upb.at[pl.ds(0, (GROUP - 1) * depth), :], level_send.at[kind])
        wait_sent(tok.at[pl.ds(0, 6 * sub), :], tok_send)
        wait_sent(tok.at[pl.ds(0, 2 * GROUP * sub), :], mate_send)
        for at_z in range(layers):
            @pl.when(z == at_z)
            def _():
                for way, reach in ((1, at_z + 1), (0, layers - at_z)):
                    if (way and at_z < layers - 1) or (not way and at_z > 0):
                        pieces = upb.at[pl.ds(0, reach * GROUP * depth), :]
                        wait_sent(pieces, piece_send.at[0, way])
                        wait_sent(downb.at[pl.ds(0, reach)], piece_send.at[1, way])

    drain_early()
    wait_sent(stage, part_send)

    @pl.when(mine_end)
    def _():
        lax.fori_loop(0, 2 * per_layer, finish, 0)

    wait_sent(peers, red_send)


def grouped(layers, tokens, norm_gain, up_weight, up_scale, down_weight, down_scale):
    rows, model = tokens.shape
    depth = up_weight.shape[0]
    if 2 * depth != COLS:
        return gathered(
            tokens, norm_gain, up_weight, up_scale, down_weight, down_scale
        )
    width = up_weight.shape[1] // GROUP
    share = model // COLS // CORES
    n = layers * GROUP
    dma = pltpu.SemaphoreType.DMA
    vmem = pl.BlockSpec(memory_space=pltpu.VMEM)
    hbm = pl.BlockSpec(memory_space=pltpu.HBM)
    ff = up_weight.shape[1]
    return pl.pallas_call(
        functools.partial(layer_kernel, layers, rows),
        out_shape=pltpu.VMEM((rows, model // CORES), jnp.bfloat16),
        in_specs=[hbm] * 6,
        out_specs=vmem,
        scratch_shapes=[
            pltpu.VMEM((1, model), jnp.float32),
            pltpu.VMEM((1, ff), jnp.float32),
            pltpu.VMEM((1, model), jnp.float32),
            pltpu.VMEM((GROUP * rows, model), jnp.bfloat16),
            pltpu.VMEM((model, width), jnp.bfloat16),
            pltpu.VMEM((layers, width, GROUP * depth), jnp.bfloat16),
            pltpu.VMEM((GROUP * rows, width), jnp.bfloat16),
            pltpu.VMEM((share, GROUP, 2, rows, COLS // 2), jnp.bfloat16),
            pltpu.VMEM((share, GROUP, 2, rows, COLS // 2), jnp.bfloat16),
            pltpu.VMEM((share, GROUP, 2, rows, COLS // 2), jnp.bfloat16),
            pltpu.VMEM((share, GROUP - 1, 2, rows, COLS // 2), jnp.bfloat16),
            pltpu.VMEM((GROUP, rows, COLS), jnp.float32),
            pltpu.VMEM((depth, GROUP * width), jnp.float32),
            pltpu.VMEM((GROUP * width, depth), jnp.float32),
            pltpu.VMEM((GROUP, depth, width), jnp.bfloat16),
            pltpu.VMEM((GROUP, width, depth), jnp.bfloat16),
            dma((7,)),
            dma((2, n)),
            dma((2, 2)),
            dma((2,)),
            dma((GROUP - 1, 2)),
            dma((GROUP - 1, 2)),
            dma((GROUP,)),
            dma((share, GROUP)),
            dma((share, 3)),
            dma((2, 2, 5)),
            dma((4,)),
        ],
        compiler_params=pltpu.CompilerParams(
            collective_id=0, has_side_effects=True, vmem_limit_bytes=60 * 2**20
        ),
    )(
        tokens, norm_gain.reshape(1, -1), up_weight, down_weight, up_scale.reshape(1, -1), down_scale
    )


def solution(mesh):
    fs, tp = mesh.shape["fs"], mesh.shape["tp"]
    if tp == CORES and fs % (2 * GROUP) == 0 and fs <= 4 * GROUP:
        body = functools.partial(grouped, fs // GROUP)
    else:
        body = gathered
    in_specs = (P("fs", None), P(), P("fs", "tp"), P("tp"), P("tp", "fs"), P())
    out_specs = P("fs", "tp")
    return jax.shard_map(
        body, mesh=mesh, in_specs=in_specs, out_specs=out_specs, check_vma=False
    )
```

```python
import functools

import jax
import jax.numpy as jnp
from jax import lax
from jax.experimental import pallas as pl
from jax.experimental.pallas import tpu as pltpu
from jax.sharding import PartitionSpec as P

MESH = pl.DeviceIdType.MESH
SIDE = 2
GROUP = SIDE * SIDE
CORES = 2
COLS = 256
STRIP = 32


def gathered(tokens, norm_gain, up_weight, up_scale, down_weight, down_scale):
    values = tokens.astype(jnp.float32)
    normed = (
        values * lax.rsqrt(jnp.mean(values * values, axis=-1, keepdims=True) + 1e-06) * norm_gain
    ).astype(jnp.bfloat16)
    up_cast = up_weight.astype(jnp.bfloat16)
    down_cast = down_weight.astype(jnp.bfloat16)
    up_full = lax.all_gather(up_cast, "fs", axis=0, tiled=True)
    pre = jnp.dot(normed, up_full, preferred_element_type=jnp.float32) * up_scale
    hidden = jnp.square(jnp.maximum(pre, 0.0)).astype(jnp.bfloat16)
    down_full = lax.all_gather(down_cast, "fs", axis=1, tiled=True)
    partial_value = jnp.dot(hidden, down_full, preferred_element_type=jnp.float32) * down_scale
    rounded = partial_value.astype(jnp.bfloat16)
    return (
        lax.psum_scatter(rounded, "tp", scatter_dimension=1, tiled=True)
        .astype(jnp.float32)
        .astype(jnp.bfloat16)
    )


def layer_kernel(
    layers, rows, tokens, gain_in, up_in, down_in, up_scale_in, down_scale_in, out,
    gain, up_scale, down_scale, tok, upb, downb, hid, stage, partner, summed, peers, own,
    up_wide, down_wide, up_cast, down_cast,
    local_sem, piece_recv, piece_send, level_send, near_recv, tok_recv, mate_recv,
    part_recv, red_recv, end_red_recv, sent,
):
    fs = lax.axis_index("fs")
    core = lax.axis_index("tp")
    z, q = fs // GROUP, fs % GROUP
    depth, width = up_in.shape[0], upb.shape[1]
    half = rows // CORES
    sub = half // 2
    units = 2 * layers
    per_layer = GROUP * depth // COLS
    per_unit = COLS // depth

    def at(r):
        return ((q // SIDE + r // SIDE) % SIDE) * SIDE + (q % SIDE + r % SIDE) % SIDE

    def chip(layer, inner):
        return (layer * GROUP + inner, core)

    mate = (fs, 1 - core)

    barrier = pltpu.get_barrier_semaphore()
    for r in (1, 2):
        pl.semaphore_signal(barrier, inc=1, device_id=chip(z, at(r)), device_id_type=MESH)
    pl.semaphore_signal(barrier, inc=1, device_id=mate, device_id_type=MESH)

    @pl.when(z > 0)
    def _():
        pl.semaphore_signal(barrier, inc=1, device_id=chip(z - 1, q), device_id_type=MESH)

    @pl.when(z < layers - 1)
    def _():
        pl.semaphore_signal(barrier, inc=1, device_id=chip(z + 1, q), device_id_type=MESH)

    def slot(kind, layer, inner):
        if kind == 0:
            return upb.at[pl.ds(pl.multiple_of((layer * GROUP + inner) * depth, depth), depth), :]
        return downb.at[layer, :, pl.ds(pl.multiple_of(inner * depth, depth), depth)]

    tok_send, mate_send, part_send, red_send = (sent.at[i] for i in range(4))

    def source(kind, inner):
        return (up_cast if kind == 0 else down_cast).at[inner]

    def remote(src, dst, send, recv, device):
        return pltpu.make_async_remote_copy(
            src_ref=src, dst_ref=dst, send_sem=send, recv_sem=recv,
            device_id=device, device_id_type=MESH,
        )

    def along(kind, layer, inner, way):
        piece = slot(kind, layer, inner)
        index = layer * GROUP + inner
        return remote(
            piece, piece, piece_send.at[kind, way], piece_recv.at[kind, index],
            chip(z + 2 * way - 1, q),
        )

    def level(r):
        return remote(
            source(1, at(r)), slot(1, z, q), level_send.at[1],
            piece_recv.at[1, fs], chip(z, at(r)),
        )

    def first_rows(h, inner=q):
        lower = (z * GROUP + inner) * depth + h * (depth // 2)
        return upb.at[pl.ds(pl.multiple_of(lower, depth // 2), depth // 2), :]

    def near_half(r, h):
        return remote(
            source(0, at(r)).at[pl.ds(h * (depth // 2), depth // 2), :], first_rows(h),
            level_send.at[0], near_recv.at[r - 1, h], chip(z, at(r)),
        )

    def half_along(inner, way, h):
        piece = first_rows(h, inner)
        index = z * GROUP + inner
        return remote(
            piece, piece, piece_send.at[0, way], piece_recv.at[0, index],
            chip(z + 2 * way - 1, q),
        )

    def each_way(kind, layer, inner, act):
        @pl.when(jnp.logical_and(layer <= z, z < layers - 1))
        def _():
            act(along(kind, layer, inner, 1))

        @pl.when(jnp.logical_and(layer >= z, z > 0))
        def _():
            act(along(kind, layer, inner, 0))

    def start(copy):
        copy.start()

    def finish_send(copy):
        copy.wait_send()

    def arrived(kind, layer, inner):
        piece = slot(kind, layer, inner)
        remote(
            piece, piece, piece_send.at[kind, 0],
            piece_recv.at[kind, layer * GROUP + inner], mate,
        ).wait_recv()

    def block(inner, side, s):
        return tok.at[pl.ds(pl.multiple_of(inner * rows + side * half + s * sub, sub), sub), :]

    def hand(r, s):
        piece = block(q, core, s)
        return remote(piece, piece, tok_send, tok_recv.at[r - 1, s], chip(z, at(r)))

    def pass_on(came, to, s):
        piece = block(at(came), core, s)
        return remote(
            piece, piece, tok_send, tok_recv.at[GROUP - 2, s], chip(z, at(to))
        )

    def tok_arrived(r, s):
        piece = block(at(r), core, s)
        remote(piece, piece, tok_send, tok_recv.at[r - 1, s], mate).wait_recv()

    def share(r, s):
        piece = block(at(r), core, s)
        return remote(piece, piece, mate_send, mate_recv.at[r], mate)

    half_at = pl.ds(pl.multiple_of(q * rows + core * half, half), half)
    mine_at = pl.ds(pl.multiple_of(core * half, half), half)

    down_copy = pltpu.make_async_copy(down_in, down_wide, local_sem.at[1])
    token_copy = pltpu.make_async_copy(tokens.at[mine_at, :], tok.at[half_at, :], local_sem.at[2])
    small = [
        pltpu.make_async_copy(gain_in, gain, local_sem.at[3]),
        pltpu.make_async_copy(up_scale_in, up_scale, local_sem.at[4]),
        pltpu.make_async_copy(down_scale_in, down_scale, local_sem.at[5]),
    ]

    def part_at(r):
        return pl.ds(pl.multiple_of(at(r) * width, width), width)

    def up_copy(r):
        return pltpu.make_async_copy(
            up_in.at[:, part_at(r)], up_wide.at[:, part_at(r)], local_sem.at[6 if r else 0]
        )

    for r in range(GROUP):
        up_copy(r).start()
    token_copy.start()
    for copy in small:
        copy.start()
    down_copy.start()
    up_copy(0).wait()
    own_rows = pl.ds(pl.multiple_of(fs * depth, depth), depth)
    upb[own_rows, :] = up_wide[:, part_at(0)].astype(upb.dtype)
    greeted = GROUP - 1 + jnp.where(z > 0, 1, 0) + jnp.where(z < layers - 1, 1, 0)
    pl.semaphore_wait(barrier, greeted)
    each_way(0, z, q, start)
    others = up_wide.at[:, pl.ds(0, (GROUP - 1) * width)]
    pltpu.make_async_copy(others, others, local_sem.at[6]).wait()
    for r in range(1, GROUP):
        up_cast[at(r)] = up_wide[:, part_at(r)].astype(up_cast.dtype)

    for r in (1, 2):
        for h in (0, 1):
            near_half(r, h).start()

    def normalize(i, carry):
        strip = pl.ds(pl.multiple_of(q * rows + core * half + i * STRIP, STRIP), STRIP)
        values = tok[strip, :].astype(jnp.float32)
        mean = jnp.mean(values * values, axis=-1, keepdims=True)
        tok[strip, :] = (values * lax.rsqrt(mean + 1e-06) * gain[...]).astype(tok.dtype)
        return carry

    token_copy.wait()
    small[0].wait()
    lax.fori_loop(0, half // STRIP, normalize, 0)
    down_copy.wait()
    own_cols = pl.ds(pl.multiple_of(q * depth, depth), depth)
    downb[z, :, own_cols] = down_wide[part_at(0), :].astype(downb.dtype)
    for r in range(1, GROUP):
        down_cast[at(r)] = down_wide[part_at(r), :].astype(down_cast.dtype)

    inside = jnp.logical_and(z > 0, z < layers - 1)

    def near(r, h):
        piece = first_rows(h, at(r))
        remote(piece, piece, level_send.at[0], near_recv.at[r - 1, h], mate).wait_recv()

        @pl.when(z < layers - 1)
        def _():
            half_along(at(r), 1, h).start()

        @pl.when(z > 0)
        def _():
            half_along(at(r), 0, h).start()

    def afar(d, r):
        for layer, there in ((z - d, z - d >= 0), (z + d, z + d < layers)):
            @pl.when(there)
            def _():
                arrived(0, layer, at(r))
                each_way(0, layer, at(r), start)

    def when_inside(d, rs):
        @pl.when(inside)
        def _():
            for r in rs:
                afar(d, r)

    near(1, 0)
    for h in (0, 1):
        near_half(3, h).start()
    hand(1, 0).start()
    hand(2, 1).start()
    hand(1, 1).start()
    hand(2, 0).start()
    for r in (1, 2, 3):
        level(r).start()
    for s in (0, 1):
        share(0, s).start()
    near(2, 0)
    near(1, 1)
    near(2, 1)
    when_inside(1, (0,))
    for h in (0, 1):
        near(3, h)
    when_inside(1, (1, 2, 3))
    tok_arrived(1, 0)
    pass_on(1, 2, 0).start()
    share(1, 0).start()
    tok_arrived(2, 1)
    pass_on(2, 1, 1).start()
    share(2, 1).start()
    for d in range(2, layers):
        when_inside(d, range(GROUP))
    for r, s in ((1, 1), (2, 0)):
        tok_arrived(r, s)
        share(r, s).start()
    for r in (1, 2, 3):
        arrived(1, z, at(r))
    for i in range(GROUP):
        each_way(1, z, i, start)

    @pl.when(jnp.logical_not(inside))
    def _():
        for d in range(1, layers):
            for r in range(GROUP):
                afar(d, r)

    def take(d, r):
        for layer, there in ((z - d, z - d >= 0), (z + d, z + d < layers)):
            @pl.when(there)
            def _():
                arrived(1, layer, r)

                @pl.when(jnp.logical_not(jnp.logical_and(
                    holds, jnp.logical_and(layer == layers - 1, r == GROUP - 1)
                )))
                def _():
                    each_way(1, layer, r, start)

    holds = jnp.logical_and(core == 1, jnp.logical_and(inside, z == 1))
    wide_n = COLS
    across = width // wide_n
    turn = jnp.where(inside, GROUP - 1, GROUP - 2)

    def first(i, carry):
        r = i // across
        b = at(r)

        @pl.when(i == turn * across)
        def _():
            for s in (0, 1):
                tok_arrived(3, s)
                share(3, s).start()

        @pl.when(i % across == 0)
        def _():
            theirs = pl.ds(pl.multiple_of(b * rows + (1 - core) * half, half), half)
            piece = tok.at[theirs, :]
            remote(piece, piece, mate_send, mate_recv.at[r], mate).wait_recv()

        m = pl.ds(pl.multiple_of(b * rows, rows), rows)
        at_n = pl.multiple_of((i % across) * wide_n, wide_n)
        pre = jnp.dot(tok[m, :], upb[:, pl.ds(at_n, wide_n)], preferred_element_type=jnp.float32)
        pre = pre * up_scale[:, pl.ds(pl.multiple_of(q * width + at_n, wide_n), wide_n)]
        hid[m, pl.ds(at_n, wide_n)] = jnp.square(jnp.maximum(pre, 0.0)).astype(hid.dtype)
        return carry

    small[1].wait()
    small[2].wait()
    lax.fori_loop(0, GROUP * across, first, 0)

    @pl.when(inside)
    def _():
        for r in range(GROUP):
            take(1, r)

    upper, lower = pl.ds(0, half), pl.ds(half, half)
    hops = ((3, upper, 2, 1), (3, lower, 2, 2), (1, upper, 0, 1), (2, lower, 1, 2),
            (1, lower, 0, 1), (2, upper, 1, 2))

    def red(u, k):
        of, part_rows, into, to = hops[k]
        return remote(
            summed.at[u, at(of), :, part_rows, :], peers.at[u, into, :, part_rows, :],
            red_send, red_recv.at[u, min(k, 2)], chip(z, at(to)),
        )

    relays = ((0, 2, upper, 5), (1, 1, lower, 4))

    def relay(u):
        for k, of, part_rows, then in relays:
            red(u, k).wait_recv()
            total = summed[u, at(of), :, part_rows, :].astype(jnp.float32)
            total = total + peers[u, 2, :, part_rows, :].astype(jnp.float32)
            summed[u, at(of), :, part_rows, :] = total.astype(summed.dtype)
            red(u, then).start()

    def unit_of(t):
        s, h = t // per_layer, t % per_layer
        layer = jnp.where(
            2 * z < layers,
            jnp.where(s <= z, z - s, s),
            jnp.where(s <= layers - 1 - z, z + s, layers - 1 - s),
        )
        unit = layer * per_layer + h
        return s, h, layer, unit, unit // (units // CORES), unit % (units // CORES)

    def part(u, b):
        return remote(
            stage.at[u, b], partner.at[u, b], part_send, part_recv.at[u, b], mate
        )

    thin = COLS // 2

    def second(t, carry):
        s, h, layer, unit, owner, u = unit_of(t)

        @pl.when(s > jnp.where(inside, 1, 0))
        def _():
            for k in range(per_unit):
                take(s, h * per_unit + k)

        cols = pl.ds(pl.multiple_of(h * COLS, COLS), COLS)
        scale = pl.ds(pl.multiple_of(unit * COLS, COLS), COLS)

        def product(b):
            m = pl.ds(pl.multiple_of(b * rows, rows), rows)
            value = jnp.dot(hid[m, :], downb[layer, :, cols], preferred_element_type=jnp.float32)
            return value * down_scale[:, scale]

        @pl.when(owner != core)
        def _():
            def away(i, c):
                b = at(GROUP - 1 - i)
                value = product(b).astype(stage.dtype)
                for e in range(2):
                    stage[u, b, e] = value[:, e * thin:(e + 1) * thin]
                part(u, b).start()
                return c

            lax.fori_loop(0, GROUP, away, 0)

        @pl.when(owner == core)
        def _():
            def mine(i, c):
                own[at(GROUP - 1 - i)] = product(at(GROUP - 1 - i))
                return c

            lax.fori_loop(0, GROUP, mine, 0)
            for r in (3, 2, 1, 0):
                b = at(r)
                part(u, b).wait_recv()
                for e in range(2):
                    total = own[b, :, e * thin:(e + 1) * thin]
                    total = total + partner[u, b, e].astype(jnp.float32)
                    summed[u, b, e] = total.astype(summed.dtype)
                for k in {3: (0, 1), 1: (2,), 2: (3,), 0: ()}[r]:
                    red(u, k).start()

        before = unit_of(jnp.maximum(t - 1, 0))

        @pl.when(jnp.logical_and(t > 0, before[4] == core))
        def _():
            relay(before[5])

        return carry

    tail = units - per_layer
    lax.fori_loop(0, tail, second, 0)
    before = unit_of(tail - 1)
    mine_end = unit_of(tail)[4] == core

    @pl.when(jnp.logical_and(before[4] == core, jnp.logical_not(mine_end)))
    def _():
        relay(before[5])

    def end_part(u, e, r):
        return remote(
            stage.at[u, at(r), e], partner.at[u, at(r), e],
            part_send, part_recv.at[u, 2 * e + (0 if r == 3 else 1)], mate,
        )

    def end_rows(k, i):
        base = hops[k][1].start
        return pl.ds(base, half) if i is None else pl.ds(base + i * sub, sub)

    def end_red(u, e, k, i=None):
        of, _, into, to = hops[k]
        come = 2 * k + i if k < 2 else 4
        return remote(
            summed.at[u, at(of), e, end_rows(k, i), :], peers.at[u, into, e, end_rows(k, i), :],
            red_send, end_red_recv.at[u % per_layer, e, come], chip(z, at(to)),
        )

    def end_relay(u, e):
        for i in range(2):
            for k, of, _, then in relays:
                end_red(u, e, k, i).wait_recv()
                total = summed[u, at(of), e, end_rows(k, i), :].astype(jnp.float32)
                total = total + peers[u, 2, e, end_rows(k, i), :].astype(jnp.float32)
                summed[u, at(of), e, end_rows(k, i), :] = total.astype(summed.dtype)
                end_red(u, e, then, i).start()

    def ending(v, carry):
        e = v % 2

        @pl.when(jnp.logical_and(holds, v == 2 * per_layer - 1))
        def _():
            each_way(1, layers - 1, GROUP - 1, start)

        s, h, layer, unit, owner, u = unit_of(tail + v // 2)

        @pl.when(s > jnp.where(inside, 1, 0))
        def _():
            take(s, h * per_unit + e)

        cols = pl.ds(pl.multiple_of(h * COLS + e * thin, thin), thin)
        scale = pl.ds(pl.multiple_of(unit * COLS + e * thin, thin), thin)

        def product(r, into):
            for i in range(CORES):
                m = pl.ds(pl.multiple_of(at(r) * rows + i * half, half), half)
                value = jnp.dot(
                    hid[m, :], downb[layer, :, cols], preferred_element_type=jnp.float32
                )
                value = value * down_scale[:, scale]
                into[pl.ds(i * half, half), :] = value.astype(into.dtype)

        @pl.when(jnp.logical_not(mine_end))
        def _():
            for r in (3, 1, 2, 0):
                product(r, stage.at[u, at(r), e])
                end_part(u, e, r).start()

        @pl.when(mine_end)
        def _():
            def compute(r):
                product(r, own.at[r, :, pl.ds(0, thin)])

            def gather(r):
                if r == 3:
                    end_part(u, e, r).wait_recv()
                elif r == 1:
                    rest = partner.at[u, pl.ds(0, GROUP - 1), e]
                    remote(rest, rest, part_send, part_recv.at[u, 2 * e + 1], mate).wait_recv()
                total = own[r, :, :thin] + partner[u, at(r), e].astype(jnp.float32)
                summed[u, at(r), e] = total.astype(summed.dtype)
                if r == 3:
                    for i in range(2):
                        for k in range(2):
                            end_red(u, e, k, i).start()
                elif r:
                    end_red(u, e, r + 1).start()

            compute(3)
            gather(3)

            @pl.when(jnp.logical_and(v == 0, before[4] == core))
            def _():
                relay(before[5])

            @pl.when(v > 0)
            def _():
                end_relay(unit_of(tail + (v - 1) // 2)[5], (v - 1) % 2)

            compute(1)
            compute(2)
            gather(1)
            compute(0)
            gather(2)
            gather(0)

        return carry

    lax.fori_loop(0, 2 * per_layer, ending, 0)

    @pl.when(mine_end)
    def _():
        end_relay(unit_of(units - 1)[5], 1)

    def last(t, carry):
        owner, u = unit_of(t)[4:]

        @pl.when(owner == core)
        def _():
            arrive = peers.at[u, pl.ds(0, 2)]
            remote(arrive, arrive, red_send, red_recv.at[u, 2], mate).wait_recv()
            for e in range(2):
                total = summed[u, q, e].astype(jnp.float32)
                for side in range(2):
                    total = total + peers[u, side, e].astype(jnp.float32)
                at_e = pl.ds(pl.multiple_of(u * COLS + e * thin, thin), thin)
                out[:, at_e] = total.astype(out.dtype)

        return carry

    lax.fori_loop(0, tail, last, 0)

    def finish(v, carry):
        e = v % 2
        u = unit_of(tail + v // 2)[5]
        arrive = peers.at[u, pl.ds(0, 2), e]
        remote(arrive, arrive, red_send, end_red_recv.at[u % per_layer, e, 4], mate).wait_recv()
        total = summed[u, q, e].astype(jnp.float32)
        for side in range(2):
            total = total + peers[u, side, e].astype(jnp.float32)
        at_e = pl.ds(pl.multiple_of(u * COLS + e * thin, thin), thin)
        out[:, at_e] = total.astype(out.dtype)
        return carry

    def wait_sent(piece, send):
        remote(piece, piece, send, piece_recv.at[0, 0], mate).wait_send()

    def drain_early():
        for kind in (0, 1):
            wait_sent(upb.at[pl.ds(0, (GROUP - 1) * depth), :], level_send.at[kind])
        wait_sent(tok.at[pl.ds(0, 6 * sub), :], tok_send)
        wait_sent(tok.at[pl.ds(0, 2 * GROUP * sub), :], mate_send)
        for at_z in range(layers):
            @pl.when(z == at_z)
            def _():
                for way, reach in ((1, at_z + 1), (0, layers - at_z)):
                    if (way and at_z < layers - 1) or (not way and at_z > 0):
                        pieces = upb.at[pl.ds(0, reach * GROUP * depth), :]
                        wait_sent(pieces, piece_send.at[0, way])
                        wait_sent(downb.at[pl.ds(0, reach)], piece_send.at[1, way])

    drain_early()
    wait_sent(stage, part_send)

    @pl.when(mine_end)
    def _():
        lax.fori_loop(0, 2 * per_layer, finish, 0)

    wait_sent(peers, red_send)


def grouped(layers, tokens, norm_gain, up_weight, up_scale, down_weight, down_scale):
    rows, model = tokens.shape
    depth = up_weight.shape[0]
    if 2 * depth != COLS:
        return gathered(
            tokens, norm_gain, up_weight, up_scale, down_weight, down_scale
        )
    width = up_weight.shape[1] // GROUP
    share = model // COLS // CORES
    n = layers * GROUP
    dma = pltpu.SemaphoreType.DMA
    vmem = pl.BlockSpec(memory_space=pltpu.VMEM)
    hbm = pl.BlockSpec(memory_space=pltpu.HBM)
    ff = up_weight.shape[1]
    return pl.pallas_call(
        functools.partial(layer_kernel, layers, rows),
        out_shape=pltpu.VMEM((rows, model // CORES), jnp.bfloat16),
        in_specs=[hbm] * 6,
        out_specs=vmem,
        scratch_shapes=[
            pltpu.VMEM((1, model), jnp.float32),
            pltpu.VMEM((1, ff), jnp.float32),
            pltpu.VMEM((1, model), jnp.float32),
            pltpu.VMEM((GROUP * rows, model), jnp.bfloat16),
            pltpu.VMEM((model, width), jnp.bfloat16),
            pltpu.VMEM((layers, width, GROUP * depth), jnp.bfloat16),
            pltpu.VMEM((GROUP * rows, width), jnp.bfloat16),
            pltpu.VMEM((share, GROUP, 2, rows, COLS // 2), jnp.bfloat16),
            pltpu.VMEM((share, GROUP, 2, rows, COLS // 2), jnp.bfloat16),
            pltpu.VMEM((share, GROUP, 2, rows, COLS // 2), jnp.bfloat16),
            pltpu.VMEM((share, GROUP - 1, 2, rows, COLS // 2), jnp.bfloat16),
            pltpu.VMEM((GROUP, rows, COLS), jnp.float32),
            pltpu.VMEM((depth, GROUP * width), jnp.float32),
            pltpu.VMEM((GROUP * width, depth), jnp.float32),
            pltpu.VMEM((GROUP, depth, width), jnp.bfloat16),
            pltpu.VMEM((GROUP, width, depth), jnp.bfloat16),
            dma((7,)),
            dma((2, n)),
            dma((2, 2)),
            dma((2,)),
            dma((GROUP - 1, 2)),
            dma((GROUP - 1, 2)),
            dma((GROUP,)),
            dma((share, GROUP)),
            dma((share, 3)),
            dma((2, 2, 5)),
            dma((4,)),
        ],
        compiler_params=pltpu.CompilerParams(
            collective_id=0, has_side_effects=True, vmem_limit_bytes=60 * 2**20
        ),
    )(
        tokens, norm_gain.reshape(1, -1), up_weight, down_weight, up_scale.reshape(1, -1), down_scale
    )


def solution(mesh):
    fs, tp = mesh.shape["fs"], mesh.shape["tp"]
    if tp == CORES and fs % (2 * GROUP) == 0 and fs <= 4 * GROUP:
        body = functools.partial(grouped, fs // GROUP)
    else:
        body = gathered
    in_specs = (P("fs", None), P(), P("fs", "tp"), P("tp"), P("tp", "fs"), P())
    out_specs = P("fs", "tp")
    return jax.shard_map(
        body, mesh=mesh, in_specs=in_specs, out_specs=out_specs, check_vma=False
    )
```

```python
import functools

import jax
import jax.numpy as jnp
from jax import lax
from jax.experimental import pallas as pl
from jax.experimental.pallas import tpu as pltpu
from jax.sharding import PartitionSpec as P

MESH = pl.DeviceIdType.MESH
SIDE = 2
GROUP = SIDE * SIDE
CORES = 2
COLS = 256
STRIP = 32


def gathered(tokens, norm_gain, up_weight, up_scale, down_weight, down_scale):
    values = tokens.astype(jnp.float32)
    normed = (
        values * lax.rsqrt(jnp.mean(values * values, axis=-1, keepdims=True) + 1e-06) * norm_gain
    ).astype(jnp.bfloat16)
    up_cast = up_weight.astype(jnp.bfloat16)
    down_cast = down_weight.astype(jnp.bfloat16)
    up_full = lax.all_gather(up_cast, "fs", axis=0, tiled=True)
    pre = jnp.dot(normed, up_full, preferred_element_type=jnp.float32) * up_scale
    hidden = jnp.square(jnp.maximum(pre, 0.0)).astype(jnp.bfloat16)
    down_full = lax.all_gather(down_cast, "fs", axis=1, tiled=True)
    partial_value = jnp.dot(hidden, down_full, preferred_element_type=jnp.float32) * down_scale
    rounded = partial_value.astype(jnp.bfloat16)
    return (
        lax.psum_scatter(rounded, "tp", scatter_dimension=1, tiled=True)
        .astype(jnp.float32)
        .astype(jnp.bfloat16)
    )


def layer_kernel(
    layers, rows, tokens, gain_in, up_in, down_in, up_scale_in, down_scale_in, out,
    gain, up_scale, down_scale, tok, upb, downb, hid, stage, partner, summed, peers, own,
    up_wide, down_wide, up_cast, down_cast,
    local_sem, piece_recv, piece_send, level_send, near_recv, tok_recv, mate_recv,
    part_recv, red_recv, end_red_recv, sent,
):
    fs = lax.axis_index("fs")
    core = lax.axis_index("tp")
    z, q = fs // GROUP, fs % GROUP
    depth, width = up_in.shape[0], upb.shape[1]
    half = rows // CORES
    sub = half // 2
    units = 2 * layers
    per_layer = GROUP * depth // COLS
    per_unit = COLS // depth

    def at(r):
        return ((q // SIDE + r // SIDE) % SIDE) * SIDE + (q % SIDE + r % SIDE) % SIDE

    def chip(layer, inner):
        return (layer * GROUP + inner, core)

    mate = (fs, 1 - core)

    barrier = pltpu.get_barrier_semaphore()
    for r in (1, 2):
        pl.semaphore_signal(barrier, inc=1, device_id=chip(z, at(r)), device_id_type=MESH)
    pl.semaphore_signal(barrier, inc=1, device_id=mate, device_id_type=MESH)

    @pl.when(z > 0)
    def _():
        pl.semaphore_signal(barrier, inc=1, device_id=chip(z - 1, q), device_id_type=MESH)

    @pl.when(z < layers - 1)
    def _():
        pl.semaphore_signal(barrier, inc=1, device_id=chip(z + 1, q), device_id_type=MESH)

    def slot(kind, layer, inner):
        if kind == 0:
            return upb.at[pl.ds(pl.multiple_of((layer * GROUP + inner) * depth, depth), depth), :]
        return downb.at[layer, :, pl.ds(pl.multiple_of(inner * depth, depth), depth)]

    tok_send, mate_send, part_send, red_send = (sent.at[i] for i in range(4))

    def source(kind, inner):
        return (up_cast if kind == 0 else down_cast).at[inner]

    def remote(src, dst, send, recv, device):
        return pltpu.make_async_remote_copy(
            src_ref=src, dst_ref=dst, send_sem=send, recv_sem=recv,
            device_id=device, device_id_type=MESH,
        )

    def along(kind, layer, inner, way):
        piece = slot(kind, layer, inner)
        index = layer * GROUP + inner
        return remote(
            piece, piece, piece_send.at[kind, way], piece_recv.at[kind, index],
            chip(z + 2 * way - 1, q),
        )

    def level(r):
        return remote(
            source(1, at(r)), slot(1, z, q), level_send.at[1],
            piece_recv.at[1, fs], chip(z, at(r)),
        )

    def first_rows(h, inner=q):
        lower = (z * GROUP + inner) * depth + h * (depth // 2)
        return upb.at[pl.ds(pl.multiple_of(lower, depth // 2), depth // 2), :]

    def near_half(r, h):
        return remote(
            source(0, at(r)).at[pl.ds(h * (depth // 2), depth // 2), :], first_rows(h),
            level_send.at[0], near_recv.at[r - 1, h], chip(z, at(r)),
        )

    def half_along(inner, way, h):
        piece = first_rows(h, inner)
        index = z * GROUP + inner
        return remote(
            piece, piece, piece_send.at[0, way], piece_recv.at[0, index],
            chip(z + 2 * way - 1, q),
        )

    def each_way(kind, layer, inner, act):
        @pl.when(jnp.logical_and(layer <= z, z < layers - 1))
        def _():
            act(along(kind, layer, inner, 1))

        @pl.when(jnp.logical_and(layer >= z, z > 0))
        def _():
            act(along(kind, layer, inner, 0))

    def start(copy):
        copy.start()

    def finish_send(copy):
        copy.wait_send()

    def arrived(kind, layer, inner):
        piece = slot(kind, layer, inner)
        remote(
            piece, piece, piece_send.at[kind, 0],
            piece_recv.at[kind, layer * GROUP + inner], mate,
        ).wait_recv()

    def block(inner, side, s):
        return tok.at[pl.ds(pl.multiple_of(inner * rows + side * half + s * sub, sub), sub), :]

    def hand(r, s):
        piece = block(q, core, s)
        return remote(piece, piece, tok_send, tok_recv.at[r - 1, s], chip(z, at(r)))

    def pass_on(came, to, s):
        piece = block(at(came), core, s)
        return remote(
            piece, piece, tok_send, tok_recv.at[GROUP - 2, s], chip(z, at(to))
        )

    def tok_arrived(r, s):
        piece = block(at(r), core, s)
        remote(piece, piece, tok_send, tok_recv.at[r - 1, s], mate).wait_recv()

    def share(r, s):
        piece = block(at(r), core, s)
        return remote(piece, piece, mate_send, mate_recv.at[r], mate)

    half_at = pl.ds(pl.multiple_of(q * rows + core * half, half), half)
    mine_at = pl.ds(pl.multiple_of(core * half, half), half)

    down_copy = pltpu.make_async_copy(down_in, down_wide, local_sem.at[1])
    token_copy = pltpu.make_async_copy(tokens.at[mine_at, :], tok.at[half_at, :], local_sem.at[2])
    small = [
        pltpu.make_async_copy(gain_in, gain, local_sem.at[3]),
        pltpu.make_async_copy(up_scale_in, up_scale, local_sem.at[4]),
        pltpu.make_async_copy(down_scale_in, down_scale, local_sem.at[5]),
    ]

    def part_at(r):
        return pl.ds(pl.multiple_of(at(r) * width, width), width)

    def up_copy(r):
        return pltpu.make_async_copy(
            up_in.at[:, part_at(r)], up_wide.at[:, part_at(r)], local_sem.at[6 if r else 0]
        )

    for r in range(GROUP):
        up_copy(r).start()
    token_copy.start()
    for copy in small:
        copy.start()
    down_copy.start()
    up_copy(0).wait()
    own_rows = pl.ds(pl.multiple_of(fs * depth, depth), depth)
    upb[own_rows, :] = up_wide[:, part_at(0)].astype(upb.dtype)
    greeted = GROUP - 1 + jnp.where(z > 0, 1, 0) + jnp.where(z < layers - 1, 1, 0)
    pl.semaphore_wait(barrier, greeted)
    each_way(0, z, q, start)
    others = up_wide.at[:, pl.ds(0, (GROUP - 1) * width)]
    pltpu.make_async_copy(others, others, local_sem.at[6]).wait()
    for r in range(1, GROUP):
        up_cast[at(r)] = up_wide[:, part_at(r)].astype(up_cast.dtype)

    for r in (1, 2):
        for h in (0, 1):
            near_half(r, h).start()

    def normalize(i, carry):
        strip = pl.ds(pl.multiple_of(q * rows + core * half + i * STRIP, STRIP), STRIP)
        values = tok[strip, :].astype(jnp.float32)
        mean = jnp.mean(values * values, axis=-1, keepdims=True)
        tok[strip, :] = (values * lax.rsqrt(mean + 1e-06) * gain[...]).astype(tok.dtype)
        return carry

    token_copy.wait()
    small[0].wait()
    lax.fori_loop(0, half // STRIP, normalize, 0)
    down_copy.wait()
    own_cols = pl.ds(pl.multiple_of(q * depth, depth), depth)
    downb[z, :, own_cols] = down_wide[part_at(0), :].astype(downb.dtype)
    for r in range(1, GROUP):
        down_cast[at(r)] = down_wide[part_at(r), :].astype(down_cast.dtype)

    inside = jnp.logical_and(z > 0, z < layers - 1)

    def near(r, h):
        piece = first_rows(h, at(r))
        remote(piece, piece, level_send.at[0], near_recv.at[r - 1, h], mate).wait_recv()

        @pl.when(z < layers - 1)
        def _():
            half_along(at(r), 1, h).start()

        @pl.when(z > 0)
        def _():
            half_along(at(r), 0, h).start()

    def afar(d, r):
        for layer, there in ((z - d, z - d >= 0), (z + d, z + d < layers)):
            @pl.when(there)
            def _():
                arrived(0, layer, at(r))
                each_way(0, layer, at(r), start)

    def when_inside(d, rs):
        @pl.when(inside)
        def _():
            for r in rs:
                afar(d, r)

    near(1, 0)
    for h in (0, 1):
        near_half(3, h).start()
    hand(1, 0).start()
    hand(2, 1).start()
    hand(1, 1).start()
    hand(2, 0).start()
    for r in (1, 2, 3):
        level(r).start()
    for s in (0, 1):
        share(0, s).start()
    near(2, 0)
    near(1, 1)
    near(2, 1)
    when_inside(1, (0,))
    for h in (0, 1):
        near(3, h)
    when_inside(1, (1, 2, 3))
    tok_arrived(1, 0)
    pass_on(1, 2, 0).start()
    share(1, 0).start()
    tok_arrived(2, 1)
    pass_on(2, 1, 1).start()
    share(2, 1).start()
    for d in range(2, layers):
        when_inside(d, range(GROUP))
    for r, s in ((1, 1), (2, 0)):
        tok_arrived(r, s)
        share(r, s).start()
    for r in (1, 2, 3):
        arrived(1, z, at(r))
    for i in range(GROUP):
        each_way(1, z, i, start)

    @pl.when(jnp.logical_not(inside))
    def _():
        for d in range(1, layers):
            for r in range(GROUP):
                afar(d, r)

    def unit_of(t):
        s, h = t // per_layer, t % per_layer
        layer = jnp.where(
            2 * z < layers,
            jnp.where(s <= z, z - s, s),
            jnp.where(s <= layers - 1 - z, z + s, layers - 1 - s),
        )
        unit = layer * per_layer + h
        return s, h, layer, unit, unit // (units // CORES), unit % (units // CORES)

    mine_end = unit_of(units - per_layer)[4] == core
    holds = jnp.logical_and(mine_end, jnp.logical_and(inside, z == 1))

    def take(d, r):
        for layer, there in ((z - d, z - d >= 0), (z + d, z + d < layers)):
            @pl.when(there)
            def _():
                arrived(1, layer, r)

                @pl.when(jnp.logical_not(jnp.logical_and(
                    holds, jnp.logical_and(layer == layers - 1, r == GROUP - 1)
                )))
                def _():
                    each_way(1, layer, r, start)

    wide_n = COLS
    across = width // wide_n
    turn = jnp.where(inside, GROUP - 1, GROUP - 2)

    def first(i, carry):
        r = i // across
        b = at(r)

        @pl.when(i == turn * across)
        def _():
            for s in (0, 1):
                tok_arrived(3, s)
                share(3, s).start()

        @pl.when(i % across == 0)
        def _():
            theirs = pl.ds(pl.multiple_of(b * rows + (1 - core) * half, half), half)
            piece = tok.at[theirs, :]
            remote(piece, piece, mate_send, mate_recv.at[r], mate).wait_recv()

        m = pl.ds(pl.multiple_of(b * rows, rows), rows)
        at_n = pl.multiple_of((i % across) * wide_n, wide_n)
        pre = jnp.dot(tok[m, :], upb[:, pl.ds(at_n, wide_n)], preferred_element_type=jnp.float32)
        pre = pre * up_scale[:, pl.ds(pl.multiple_of(q * width + at_n, wide_n), wide_n)]
        hid[m, pl.ds(at_n, wide_n)] = jnp.square(jnp.maximum(pre, 0.0)).astype(hid.dtype)
        return carry

    small[1].wait()
    small[2].wait()
    lax.fori_loop(0, GROUP * across, first, 0)

    @pl.when(inside)
    def _():
        for r in range(GROUP):
            take(1, r)

    upper, lower = pl.ds(0, half), pl.ds(half, half)
    hops = ((3, upper, 2, 1), (3, lower, 2, 2), (1, upper, 0, 1), (2, lower, 1, 2),
            (1, lower, 0, 1), (2, upper, 1, 2))

    def red(u, k):
        of, part_rows, into, to = hops[k]
        return remote(
            summed.at[u, at(of), :, part_rows, :], peers.at[u, into, :, part_rows, :],
            red_send, red_recv.at[u, min(k, 2)], chip(z, at(to)),
        )

    relays = ((0, 2, upper, 5), (1, 1, lower, 4))

    def relay(u):
        for k, of, part_rows, then in relays:
            red(u, k).wait_recv()
            total = summed[u, at(of), :, part_rows, :].astype(jnp.float32)
            total = total + peers[u, 2, :, part_rows, :].astype(jnp.float32)
            summed[u, at(of), :, part_rows, :] = total.astype(summed.dtype)
            red(u, then).start()

    def part(u, b):
        return remote(
            stage.at[u, b], partner.at[u, b], part_send, part_recv.at[u, b], mate
        )

    thin = COLS // 2

    def second(t, carry):
        s, h, layer, unit, owner, u = unit_of(t)

        @pl.when(s > jnp.where(inside, 1, 0))
        def _():
            for k in range(per_unit):
                take(s, h * per_unit + k)

        cols = pl.ds(pl.multiple_of(h * COLS, COLS), COLS)
        scale = pl.ds(pl.multiple_of(unit * COLS, COLS), COLS)

        def product(b):
            m = pl.ds(pl.multiple_of(b * rows, rows), rows)
            value = jnp.dot(hid[m, :], downb[layer, :, cols], preferred_element_type=jnp.float32)
            return value * down_scale[:, scale]

        @pl.when(owner != core)
        def _():
            def away(i, c):
                b = at(GROUP - 1 - i)
                value = product(b).astype(stage.dtype)
                for e in range(2):
                    stage[u, b, e] = value[:, e * thin:(e + 1) * thin]
                part(u, b).start()
                return c

            lax.fori_loop(0, GROUP, away, 0)

        @pl.when(owner == core)
        def _():
            def mine(i, c):
                own[at(GROUP - 1 - i)] = product(at(GROUP - 1 - i))
                return c

            lax.fori_loop(0, GROUP, mine, 0)
            for r in (3, 2, 1, 0):
                b = at(r)
                part(u, b).wait_recv()
                for e in range(2):
                    total = own[b, :, e * thin:(e + 1) * thin]
                    total = total + partner[u, b, e].astype(jnp.float32)
                    summed[u, b, e] = total.astype(summed.dtype)
                for k in {3: (0, 1), 1: (2,), 2: (3,), 0: ()}[r]:
                    red(u, k).start()

        before = unit_of(jnp.maximum(t - 1, 0))

        @pl.when(jnp.logical_and(t > 0, before[4] == core))
        def _():
            relay(before[5])

        return carry

    tail = units - per_layer
    lax.fori_loop(0, tail, second, 0)
    before = unit_of(tail - 1)

    @pl.when(jnp.logical_and(before[4] == core, jnp.logical_not(mine_end)))
    def _():
        relay(before[5])

    def end_part(u, e, r):
        return remote(
            stage.at[u, at(r), e], partner.at[u, at(r), e],
            part_send, part_recv.at[u, 2 * e + (0 if r == 3 else 1)], mate,
        )

    def end_rows(k, i):
        base = hops[k][1].start
        return pl.ds(base, half) if i is None else pl.ds(base + i * sub, sub)

    def end_red(u, e, k, i=None):
        of, _, into, to = hops[k]
        come = 2 * k + i if k < 2 else 4
        return remote(
            summed.at[u, at(of), e, end_rows(k, i), :], peers.at[u, into, e, end_rows(k, i), :],
            red_send, end_red_recv.at[u % per_layer, e, come], chip(z, at(to)),
        )

    def end_relay(u, e):
        for i in range(2):
            for k, of, _, then in relays:
                end_red(u, e, k, i).wait_recv()
                total = summed[u, at(of), e, end_rows(k, i), :].astype(jnp.float32)
                total = total + peers[u, 2, e, end_rows(k, i), :].astype(jnp.float32)
                summed[u, at(of), e, end_rows(k, i), :] = total.astype(summed.dtype)
                end_red(u, e, then, i).start()

    def ending(v, carry):
        e = v % 2

        def release(when):
            @pl.when(jnp.logical_and(when, jnp.logical_and(holds, v == 2 * per_layer - 1)))
            def _():
                each_way(1, layers - 1, GROUP - 1, start)

        corner = q == GROUP - 1
        release(jnp.logical_not(corner))

        s, h, layer, unit, owner, u = unit_of(tail + v // 2)

        @pl.when(s > jnp.where(inside, 1, 0))
        def _():
            take(s, h * per_unit + e)

        cols = pl.ds(pl.multiple_of(h * COLS + e * thin, thin), thin)
        scale = pl.ds(pl.multiple_of(unit * COLS + e * thin, thin), thin)

        def product(r, into):
            for i in range(CORES):
                m = pl.ds(pl.multiple_of(at(r) * rows + i * half, half), half)
                value = jnp.dot(
                    hid[m, :], downb[layer, :, cols], preferred_element_type=jnp.float32
                )
                value = value * down_scale[:, scale]
                into[pl.ds(i * half, half), :] = value.astype(into.dtype)

        @pl.when(jnp.logical_not(mine_end))
        def _():
            for r in (3, 1, 2, 0):
                product(r, stage.at[u, at(r), e])
                end_part(u, e, r).start()

        @pl.when(mine_end)
        def _():
            def compute(r):
                product(r, own.at[r, :, pl.ds(0, thin)])

            def gather(r):
                if r == 3:
                    end_part(u, e, r).wait_recv()
                elif r == 1:
                    rest = partner.at[u, pl.ds(0, GROUP - 1), e]
                    remote(rest, rest, part_send, part_recv.at[u, 2 * e + 1], mate).wait_recv()
                total = own[r, :, :thin] + partner[u, at(r), e].astype(jnp.float32)
                summed[u, at(r), e] = total.astype(summed.dtype)
                if r == 3:
                    for i in range(2):
                        for k in range(2):
                            end_red(u, e, k, i).start()
                elif r:
                    end_red(u, e, r + 1).start()

            compute(3)
            gather(3)
            release(corner)

            @pl.when(jnp.logical_and(v == 0, before[4] == core))
            def _():
                relay(before[5])

            @pl.when(v > 0)
            def _():
                end_relay(unit_of(tail + (v - 1) // 2)[5], (v - 1) % 2)

            compute(1)
            compute(2)
            gather(1)
            compute(0)
            gather(2)
            gather(0)

        return carry

    lax.fori_loop(0, 2 * per_layer, ending, 0)

    @pl.when(mine_end)
    def _():
        end_relay(unit_of(units - 1)[5], 1)

    def last(t, carry):
        owner, u = unit_of(t)[4:]

        @pl.when(owner == core)
        def _():
            arrive = peers.at[u, pl.ds(0, 2)]
            remote(arrive, arrive, red_send, red_recv.at[u, 2], mate).wait_recv()
            for e in range(2):
                total = summed[u, q, e].astype(jnp.float32)
                for side in range(2):
                    total = total + peers[u, side, e].astype(jnp.float32)
                at_e = pl.ds(pl.multiple_of(u * COLS + e * thin, thin), thin)
                out[:, at_e] = total.astype(out.dtype)

        return carry

    lax.fori_loop(0, tail, last, 0)

    def finish(v, carry):
        e = v % 2
        u = unit_of(tail + v // 2)[5]
        arrive = peers.at[u, pl.ds(0, 2), e]
        remote(arrive, arrive, red_send, end_red_recv.at[u % per_layer, e, 4], mate).wait_recv()
        total = summed[u, q, e].astype(jnp.float32)
        for side in range(2):
            total = total + peers[u, side, e].astype(jnp.float32)
        at_e = pl.ds(pl.multiple_of(u * COLS + e * thin, thin), thin)
        out[:, at_e] = total.astype(out.dtype)
        return carry

    def wait_sent(piece, send):
        remote(piece, piece, send, piece_recv.at[0, 0], mate).wait_send()

    def drain_early():
        for kind in (0, 1):
            wait_sent(upb.at[pl.ds(0, (GROUP - 1) * depth), :], level_send.at[kind])
        wait_sent(tok.at[pl.ds(0, 6 * sub), :], tok_send)
        wait_sent(tok.at[pl.ds(0, 2 * GROUP * sub), :], mate_send)
        for at_z in range(layers):
            @pl.when(z == at_z)
            def _():
                for way, reach in ((1, at_z + 1), (0, layers - at_z)):
                    if (way and at_z < layers - 1) or (not way and at_z > 0):
                        pieces = upb.at[pl.ds(0, reach * GROUP * depth), :]
                        wait_sent(pieces, piece_send.at[0, way])
                        wait_sent(downb.at[pl.ds(0, reach)], piece_send.at[1, way])

    drain_early()
    wait_sent(stage, part_send)

    @pl.when(mine_end)
    def _():
        lax.fori_loop(0, 2 * per_layer, finish, 0)

    wait_sent(peers, red_send)


def grouped(layers, tokens, norm_gain, up_weight, up_scale, down_weight, down_scale):
    rows, model = tokens.shape
    depth = up_weight.shape[0]
    if 2 * depth != COLS:
        return gathered(
            tokens, norm_gain, up_weight, up_scale, down_weight, down_scale
        )
    width = up_weight.shape[1] // GROUP
    share = model // COLS // CORES
    n = layers * GROUP
    dma = pltpu.SemaphoreType.DMA
    vmem = pl.BlockSpec(memory_space=pltpu.VMEM)
    hbm = pl.BlockSpec(memory_space=pltpu.HBM)
    ff = up_weight.shape[1]
    return pl.pallas_call(
        functools.partial(layer_kernel, layers, rows),
        out_shape=pltpu.VMEM((rows, model // CORES), jnp.bfloat16),
        in_specs=[hbm] * 6,
        out_specs=vmem,
        scratch_shapes=[
            pltpu.VMEM((1, model), jnp.float32),
            pltpu.VMEM((1, ff), jnp.float32),
            pltpu.VMEM((1, model), jnp.float32),
            pltpu.VMEM((GROUP * rows, model), jnp.bfloat16),
            pltpu.VMEM((model, width), jnp.bfloat16),
            pltpu.VMEM((layers, width, GROUP * depth), jnp.bfloat16),
            pltpu.VMEM((GROUP * rows, width), jnp.bfloat16),
            pltpu.VMEM((share, GROUP, 2, rows, COLS // 2), jnp.bfloat16),
            pltpu.VMEM((share, GROUP, 2, rows, COLS // 2), jnp.bfloat16),
            pltpu.VMEM((share, GROUP, 2, rows, COLS // 2), jnp.bfloat16),
            pltpu.VMEM((share, GROUP - 1, 2, rows, COLS // 2), jnp.bfloat16),
            pltpu.VMEM((GROUP, rows, COLS), jnp.float32),
            pltpu.VMEM((depth, GROUP * width), jnp.float32),
            pltpu.VMEM((GROUP * width, depth), jnp.float32),
            pltpu.VMEM((GROUP, depth, width), jnp.bfloat16),
            pltpu.VMEM((GROUP, width, depth), jnp.bfloat16),
            dma((7,)),
            dma((2, n)),
            dma((2, 2)),
            dma((2,)),
            dma((GROUP - 1, 2)),
            dma((GROUP - 1, 2)),
            dma((GROUP,)),
            dma((share, GROUP)),
            dma((share, 3)),
            dma((2, 2, 5)),
            dma((4,)),
        ],
        compiler_params=pltpu.CompilerParams(
            collective_id=0, has_side_effects=True, vmem_limit_bytes=60 * 2**20
        ),
    )(
        tokens, norm_gain.reshape(1, -1), up_weight, down_weight, up_scale.reshape(1, -1), down_scale
    )


def solution(mesh):
    fs, tp = mesh.shape["fs"], mesh.shape["tp"]
    if tp == CORES and fs % (2 * GROUP) == 0 and fs <= 4 * GROUP:
        body = functools.partial(grouped, fs // GROUP)
    else:
        body = gathered
    in_specs = (P("fs", None), P(), P("fs", "tp"), P("tp"), P("tp", "fs"), P())
    out_specs = P("fs", "tp")
    return jax.shard_map(
        body, mesh=mesh, in_specs=in_specs, out_specs=out_specs, check_vma=False
    )
```

```python
import functools

import jax
import jax.numpy as jnp
from jax import lax
from jax.experimental import pallas as pl
from jax.experimental.pallas import tpu as pltpu
from jax.sharding import PartitionSpec as P

MESH = pl.DeviceIdType.MESH
SIDE = 2
GROUP = SIDE * SIDE
CORES = 2
COLS = 256
STRIP = 32


def gathered(tokens, norm_gain, up_weight, up_scale, down_weight, down_scale):
    values = tokens.astype(jnp.float32)
    normed = (
        values * lax.rsqrt(jnp.mean(values * values, axis=-1, keepdims=True) + 1e-06) * norm_gain
    ).astype(jnp.bfloat16)
    up_cast = up_weight.astype(jnp.bfloat16)
    down_cast = down_weight.astype(jnp.bfloat16)
    up_full = lax.all_gather(up_cast, "fs", axis=0, tiled=True)
    pre = jnp.dot(normed, up_full, preferred_element_type=jnp.float32) * up_scale
    hidden = jnp.square(jnp.maximum(pre, 0.0)).astype(jnp.bfloat16)
    down_full = lax.all_gather(down_cast, "fs", axis=1, tiled=True)
    partial_value = jnp.dot(hidden, down_full, preferred_element_type=jnp.float32) * down_scale
    rounded = partial_value.astype(jnp.bfloat16)
    return (
        lax.psum_scatter(rounded, "tp", scatter_dimension=1, tiled=True)
        .astype(jnp.float32)
        .astype(jnp.bfloat16)
    )


def layer_kernel(
    layers, rows, tokens, gain_in, up_in, down_in, up_scale_in, down_scale_in, out,
    gain, up_scale, down_scale, tok, upb, downb, hid, stage, partner, summed, peers, own,
    up_wide, down_wide, up_cast, down_cast,
    local_sem, piece_recv, piece_send, level_send, near_recv, tok_recv, mate_recv,
    part_recv, red_recv, end_red_recv, sent,
):
    fs = lax.axis_index("fs")
    core = lax.axis_index("tp")
    z, q = fs // GROUP, fs % GROUP
    depth, width = up_in.shape[0], upb.shape[1]
    half = rows // CORES
    sub = half // 2
    units = 2 * layers
    per_layer = GROUP * depth // COLS
    per_unit = COLS // depth

    def at(r):
        return ((q // SIDE + r // SIDE) % SIDE) * SIDE + (q % SIDE + r % SIDE) % SIDE

    def chip(layer, inner):
        return (layer * GROUP + inner, core)

    mate = (fs, 1 - core)

    barrier = pltpu.get_barrier_semaphore()
    for r in (1, 2):
        pl.semaphore_signal(barrier, inc=1, device_id=chip(z, at(r)), device_id_type=MESH)
    pl.semaphore_signal(barrier, inc=1, device_id=mate, device_id_type=MESH)

    @pl.when(z > 0)
    def _():
        pl.semaphore_signal(barrier, inc=1, device_id=chip(z - 1, q), device_id_type=MESH)

    @pl.when(z < layers - 1)
    def _():
        pl.semaphore_signal(barrier, inc=1, device_id=chip(z + 1, q), device_id_type=MESH)

    def slot(kind, layer, inner):
        if kind == 0:
            return upb.at[pl.ds(pl.multiple_of((layer * GROUP + inner) * depth, depth), depth), :]
        return downb.at[layer, :, pl.ds(pl.multiple_of(inner * depth, depth), depth)]

    tok_send, mate_send, part_send, red_send = (sent.at[i] for i in range(4))

    def source(kind, inner):
        return (up_cast if kind == 0 else down_cast).at[inner]

    def remote(src, dst, send, recv, device):
        return pltpu.make_async_remote_copy(
            src_ref=src, dst_ref=dst, send_sem=send, recv_sem=recv,
            device_id=device, device_id_type=MESH,
        )

    def along(kind, layer, inner, way):
        piece = slot(kind, layer, inner)
        index = layer * GROUP + inner
        return remote(
            piece, piece, piece_send.at[kind, way], piece_recv.at[kind, index],
            chip(z + 2 * way - 1, q),
        )

    def level(r):
        return remote(
            source(1, at(r)), slot(1, z, q), level_send.at[1],
            piece_recv.at[1, fs], chip(z, at(r)),
        )

    def first_rows(h, inner=q):
        lower = (z * GROUP + inner) * depth + h * (depth // 2)
        return upb.at[pl.ds(pl.multiple_of(lower, depth // 2), depth // 2), :]

    def near_half(r, h):
        return remote(
            source(0, at(r)).at[pl.ds(h * (depth // 2), depth // 2), :], first_rows(h),
            level_send.at[0], near_recv.at[r - 1, h], chip(z, at(r)),
        )

    def half_along(inner, way, h):
        piece = first_rows(h, inner)
        index = z * GROUP + inner
        return remote(
            piece, piece, piece_send.at[0, way], piece_recv.at[0, index],
            chip(z + 2 * way - 1, q),
        )

    def each_way(kind, layer, inner, act):
        @pl.when(jnp.logical_and(layer <= z, z < layers - 1))
        def _():
            act(along(kind, layer, inner, 1))

        @pl.when(jnp.logical_and(layer >= z, z > 0))
        def _():
            act(along(kind, layer, inner, 0))

    def start(copy):
        copy.start()

    def finish_send(copy):
        copy.wait_send()

    def arrived(kind, layer, inner):
        piece = slot(kind, layer, inner)
        remote(
            piece, piece, piece_send.at[kind, 0],
            piece_recv.at[kind, layer * GROUP + inner], mate,
        ).wait_recv()

    def block(inner, side, s):
        return tok.at[pl.ds(pl.multiple_of(inner * rows + side * half + s * sub, sub), sub), :]

    def hand(r, s):
        piece = block(q, core, s)
        return remote(piece, piece, tok_send, tok_recv.at[r - 1, s], chip(z, at(r)))

    def pass_on(came, to, s):
        piece = block(at(came), core, s)
        return remote(
            piece, piece, tok_send, tok_recv.at[GROUP - 2, s], chip(z, at(to))
        )

    def tok_arrived(r, s):
        piece = block(at(r), core, s)
        remote(piece, piece, tok_send, tok_recv.at[r - 1, s], mate).wait_recv()

    def share(r, s):
        piece = block(at(r), core, s)
        return remote(piece, piece, mate_send, mate_recv.at[r], mate)

    half_at = pl.ds(pl.multiple_of(q * rows + core * half, half), half)
    mine_at = pl.ds(pl.multiple_of(core * half, half), half)

    down_copy = pltpu.make_async_copy(down_in, down_wide, local_sem.at[1])
    token_copy = pltpu.make_async_copy(tokens.at[mine_at, :], tok.at[half_at, :], local_sem.at[2])
    small = [
        pltpu.make_async_copy(gain_in, gain, local_sem.at[3]),
        pltpu.make_async_copy(up_scale_in, up_scale, local_sem.at[4]),
        pltpu.make_async_copy(down_scale_in, down_scale, local_sem.at[5]),
    ]

    def part_at(r):
        return pl.ds(pl.multiple_of(at(r) * width, width), width)

    def up_copy(r):
        return pltpu.make_async_copy(
            up_in.at[:, part_at(r)], up_wide.at[:, part_at(r)], local_sem.at[6 if r else 0]
        )

    for r in range(GROUP):
        up_copy(r).start()
    token_copy.start()
    for copy in small:
        copy.start()
    down_copy.start()
    up_copy(0).wait()
    own_rows = pl.ds(pl.multiple_of(fs * depth, depth), depth)
    upb[own_rows, :] = up_wide[:, part_at(0)].astype(upb.dtype)
    greeted = GROUP - 1 + jnp.where(z > 0, 1, 0) + jnp.where(z < layers - 1, 1, 0)
    pl.semaphore_wait(barrier, greeted)
    each_way(0, z, q, start)
    others = up_wide.at[:, pl.ds(0, (GROUP - 1) * width)]
    pltpu.make_async_copy(others, others, local_sem.at[6]).wait()
    for r in range(1, GROUP):
        up_cast[at(r)] = up_wide[:, part_at(r)].astype(up_cast.dtype)

    for r in (1, 2):
        for h in (0, 1):
            near_half(r, h).start()

    def normalize(i, carry):
        strip = pl.ds(pl.multiple_of(q * rows + core * half + i * STRIP, STRIP), STRIP)
        values = tok[strip, :].astype(jnp.float32)
        mean = jnp.mean(values * values, axis=-1, keepdims=True)
        tok[strip, :] = (values * lax.rsqrt(mean + 1e-06) * gain[...]).astype(tok.dtype)
        return carry

    token_copy.wait()
    small[0].wait()
    lax.fori_loop(0, half // STRIP, normalize, 0)
    down_copy.wait()
    own_cols = pl.ds(pl.multiple_of(q * depth, depth), depth)
    downb[z, :, own_cols] = down_wide[part_at(0), :].astype(downb.dtype)
    for r in range(1, GROUP):
        down_cast[at(r)] = down_wide[part_at(r), :].astype(down_cast.dtype)

    inside = jnp.logical_and(z > 0, z < layers - 1)

    def near(r, h):
        piece = first_rows(h, at(r))
        remote(piece, piece, level_send.at[0], near_recv.at[r - 1, h], mate).wait_recv()

        @pl.when(z < layers - 1)
        def _():
            half_along(at(r), 1, h).start()

        @pl.when(z > 0)
        def _():
            half_along(at(r), 0, h).start()

    def afar(d, r):
        for layer, there in ((z - d, z - d >= 0), (z + d, z + d < layers)):
            @pl.when(there)
            def _():
                arrived(0, layer, at(r))
                each_way(0, layer, at(r), start)

    def when_inside(d, rs):
        @pl.when(inside)
        def _():
            for r in rs:
                afar(d, r)

    near(1, 0)
    for h in (0, 1):
        near_half(3, h).start()
    hand(1, 0).start()
    hand(2, 1).start()
    hand(1, 1).start()
    hand(2, 0).start()
    for r in (1, 2, 3):
        level(r).start()
    for s in (0, 1):
        share(0, s).start()
    near(2, 0)
    near(1, 1)
    near(2, 1)
    when_inside(1, (0,))
    for h in (0, 1):
        near(3, h)
    when_inside(1, (1, 2, 3))
    tok_arrived(1, 0)
    pass_on(1, 2, 0).start()
    share(1, 0).start()
    tok_arrived(2, 1)
    pass_on(2, 1, 1).start()
    share(2, 1).start()
    for d in range(2, layers):
        when_inside(d, range(GROUP))
    for r, s in ((1, 1), (2, 0)):
        tok_arrived(r, s)
        share(r, s).start()
    for r in (1, 2, 3):
        arrived(1, z, at(r))
    for i in range(GROUP):
        each_way(1, z, i, start)

    @pl.when(jnp.logical_not(inside))
    def _():
        for d in range(1, layers):
            for r in range(GROUP):
                afar(d, r)

    def unit_of(t):
        s, h = t // per_layer, t % per_layer
        layer = jnp.where(
            2 * z < layers,
            jnp.where(s <= z, z - s, s),
            jnp.where(s <= layers - 1 - z, z + s, layers - 1 - s),
        )
        unit = layer * per_layer + h
        return s, h, layer, unit, unit // (units // CORES), unit % (units // CORES)

    mine_end = unit_of(units - per_layer)[4] == core
    holds = jnp.logical_and(mine_end, jnp.logical_and(inside, z == 1))

    def take(d, r):
        for layer, there in ((z - d, z - d >= 0), (z + d, z + d < layers)):
            @pl.when(there)
            def _():
                arrived(1, layer, r)

                @pl.when(jnp.logical_not(jnp.logical_and(
                    holds, jnp.logical_and(layer == layers - 1, r == GROUP - 1)
                )))
                def _():
                    each_way(1, layer, r, start)

    wide_n = COLS
    across = width // wide_n
    turn = jnp.where(inside, GROUP - 1, GROUP - 2)

    def first(i, carry):
        r = i // across
        b = at(r)

        @pl.when(i == turn * across)
        def _():
            for s in (0, 1):
                tok_arrived(3, s)
                share(3, s).start()

        @pl.when(i % across == 0)
        def _():
            theirs = pl.ds(pl.multiple_of(b * rows + (1 - core) * half, half), half)
            piece = tok.at[theirs, :]
            remote(piece, piece, mate_send, mate_recv.at[r], mate).wait_recv()

        m = pl.ds(pl.multiple_of(b * rows, rows), rows)
        at_n = pl.multiple_of((i % across) * wide_n, wide_n)
        pre = jnp.dot(tok[m, :], upb[:, pl.ds(at_n, wide_n)], preferred_element_type=jnp.float32)
        pre = pre * up_scale[:, pl.ds(pl.multiple_of(q * width + at_n, wide_n), wide_n)]
        hid[m, pl.ds(at_n, wide_n)] = jnp.square(jnp.maximum(pre, 0.0)).astype(hid.dtype)
        return carry

    small[1].wait()
    small[2].wait()
    lax.fori_loop(0, GROUP * across, first, 0)

    @pl.when(inside)
    def _():
        for r in range(GROUP):
            take(1, r)

    upper, lower = pl.ds(0, half), pl.ds(half, half)
    hops = ((3, upper, 2, 1), (3, lower, 2, 2), (1, upper, 0, 1), (2, lower, 1, 2),
            (1, lower, 0, 1), (2, upper, 1, 2))

    def red(u, k):
        of, part_rows, into, to = hops[k]
        return remote(
            summed.at[u, at(of), :, part_rows, :], peers.at[u, into, :, part_rows, :],
            red_send, red_recv.at[u, min(k, 2)], chip(z, at(to)),
        )

    relays = ((0, 2, upper, 5), (1, 1, lower, 4))

    def relay(u):
        for k, of, part_rows, then in relays:
            red(u, k).wait_recv()
            total = summed[u, at(of), :, part_rows, :].astype(jnp.float32)
            total = total + peers[u, 2, :, part_rows, :].astype(jnp.float32)
            summed[u, at(of), :, part_rows, :] = total.astype(summed.dtype)
            red(u, then).start()

    def part(u, b):
        return remote(
            stage.at[u, b], partner.at[u, b], part_send, part_recv.at[u, b], mate
        )

    thin = COLS // 2

    def second(t, carry):
        s, h, layer, unit, owner, u = unit_of(t)

        @pl.when(s > jnp.where(inside, 1, 0))
        def _():
            for k in range(per_unit):
                take(s, h * per_unit + k)

        cols = pl.ds(pl.multiple_of(h * COLS, COLS), COLS)
        scale = pl.ds(pl.multiple_of(unit * COLS, COLS), COLS)

        def product(b):
            m = pl.ds(pl.multiple_of(b * rows, rows), rows)
            value = jnp.dot(hid[m, :], downb[layer, :, cols], preferred_element_type=jnp.float32)
            return value * down_scale[:, scale]

        @pl.when(owner != core)
        def _():
            def away(i, c):
                b = at(GROUP - 1 - i)
                value = product(b).astype(stage.dtype)
                for e in range(2):
                    stage[u, b, e] = value[:, e * thin:(e + 1) * thin]
                part(u, b).start()
                return c

            lax.fori_loop(0, GROUP, away, 0)

        @pl.when(owner == core)
        def _():
            def mine(i, c):
                own[at(GROUP - 1 - i)] = product(at(GROUP - 1 - i))
                return c

            lax.fori_loop(0, GROUP, mine, 0)
            for r in (3, 2, 1, 0):
                b = at(r)
                part(u, b).wait_recv()
                for e in range(2):
                    total = own[b, :, e * thin:(e + 1) * thin]
                    total = total + partner[u, b, e].astype(jnp.float32)
                    summed[u, b, e] = total.astype(summed.dtype)
                for k in {3: (0, 1), 1: (2,), 2: (3,), 0: ()}[r]:
                    red(u, k).start()

        before = unit_of(jnp.maximum(t - 1, 0))

        @pl.when(jnp.logical_and(t > 0, before[4] == core))
        def _():
            relay(before[5])

        return carry

    tail = units - per_layer
    lax.fori_loop(0, tail, second, 0)
    before = unit_of(tail - 1)

    @pl.when(jnp.logical_and(before[4] == core, jnp.logical_not(mine_end)))
    def _():
        relay(before[5])

    def end_part(u, e, r):
        return remote(
            stage.at[u, at(r), e], partner.at[u, at(r), e],
            part_send, part_recv.at[u, 2 * e + (0 if r == 3 else 1)], mate,
        )

    def end_rows(k, i):
        base = hops[k][1].start
        return pl.ds(base, half) if i is None else pl.ds(base + i * sub, sub)

    def end_red(u, e, k, i=None):
        of, _, into, to = hops[k]
        come = 2 * k + i if k < 2 else 4
        return remote(
            summed.at[u, at(of), e, end_rows(k, i), :], peers.at[u, into, e, end_rows(k, i), :],
            red_send, end_red_recv.at[u % per_layer, e, come], chip(z, at(to)),
        )

    def end_relay(u, e):
        for i in range(2):
            for k, of, _, then in relays:
                end_red(u, e, k, i).wait_recv()
                total = summed[u, at(of), e, end_rows(k, i), :].astype(jnp.float32)
                total = total + peers[u, 2, e, end_rows(k, i), :].astype(jnp.float32)
                summed[u, at(of), e, end_rows(k, i), :] = total.astype(summed.dtype)
                end_red(u, e, then, i).start()

    def ending(v, carry):
        e = v % 2

        def release(when):
            @pl.when(jnp.logical_and(when, jnp.logical_and(holds, v == 2 * per_layer - 1)))
            def _():
                each_way(1, layers - 1, GROUP - 1, start)

        corner = q == GROUP - 1
        release(jnp.logical_not(corner))

        s, h, layer, unit, owner, u = unit_of(tail + v // 2)

        @pl.when(s > jnp.where(inside, 1, 0))
        def _():
            take(s, h * per_unit + e)

        cols = pl.ds(pl.multiple_of(h * COLS + e * thin, thin), thin)
        scale = pl.ds(pl.multiple_of(unit * COLS + e * thin, thin), thin)

        def product(r, into):
            for i in range(CORES):
                m = pl.ds(pl.multiple_of(at(r) * rows + i * half, half), half)
                value = jnp.dot(
                    hid[m, :], downb[layer, :, cols], preferred_element_type=jnp.float32
                )
                value = value * down_scale[:, scale]
                into[pl.ds(i * half, half), :] = value.astype(into.dtype)

        @pl.when(jnp.logical_not(mine_end))
        def _():
            for r in (3, 1, 2, 0):
                product(r, stage.at[u, at(r), e])
                end_part(u, e, r).start()

        @pl.when(mine_end)
        def _():
            def compute(r):
                product(r, own.at[r, :, pl.ds(0, thin)])

            def gather(r):
                if r == 3:
                    end_part(u, e, r).wait_recv()
                elif r == 1:
                    rest = partner.at[u, pl.ds(0, GROUP - 1), e]
                    remote(rest, rest, part_send, part_recv.at[u, 2 * e + 1], mate).wait_recv()
                total = own[r, :, :thin] + partner[u, at(r), e].astype(jnp.float32)
                summed[u, at(r), e] = total.astype(summed.dtype)
                if r == 3:
                    for i in range(2):
                        for k in range(2):
                            end_red(u, e, k, i).start()
                elif r:
                    end_red(u, e, r + 1).start()

            @pl.when(jnp.logical_and(v == 0, before[4] == core))
            def _():
                relay(before[5])

            @pl.when(v > 0)
            def _():
                end_relay(unit_of(tail + (v - 1) // 2)[5], (v - 1) % 2)

            compute(3)
            gather(3)
            release(corner)
            compute(1)
            compute(2)
            gather(1)
            compute(0)
            gather(2)
            gather(0)

        return carry

    lax.fori_loop(0, 2 * per_layer, ending, 0)

    @pl.when(mine_end)
    def _():
        end_relay(unit_of(units - 1)[5], 1)

    def last(t, carry):
        owner, u = unit_of(t)[4:]

        @pl.when(owner == core)
        def _():
            arrive = peers.at[u, pl.ds(0, 2)]
            remote(arrive, arrive, red_send, red_recv.at[u, 2], mate).wait_recv()
            for e in range(2):
                total = summed[u, q, e].astype(jnp.float32)
                for side in range(2):
                    total = total + peers[u, side, e].astype(jnp.float32)
                at_e = pl.ds(pl.multiple_of(u * COLS + e * thin, thin), thin)
                out[:, at_e] = total.astype(out.dtype)

        return carry

    lax.fori_loop(0, tail, last, 0)

    def finish(v, carry):
        e = v % 2
        u = unit_of(tail + v // 2)[5]
        arrive = peers.at[u, pl.ds(0, 2), e]
        remote(arrive, arrive, red_send, end_red_recv.at[u % per_layer, e, 4], mate).wait_recv()
        total = summed[u, q, e].astype(jnp.float32)
        for side in range(2):
            total = total + peers[u, side, e].astype(jnp.float32)
        at_e = pl.ds(pl.multiple_of(u * COLS + e * thin, thin), thin)
        out[:, at_e] = total.astype(out.dtype)
        return carry

    def wait_sent(piece, send):
        remote(piece, piece, send, piece_recv.at[0, 0], mate).wait_send()

    def drain_early():
        for kind in (0, 1):
            wait_sent(upb.at[pl.ds(0, (GROUP - 1) * depth), :], level_send.at[kind])
        wait_sent(tok.at[pl.ds(0, 6 * sub), :], tok_send)
        wait_sent(tok.at[pl.ds(0, 2 * GROUP * sub), :], mate_send)
        for at_z in range(layers):
            @pl.when(z == at_z)
            def _():
                for way, reach in ((1, at_z + 1), (0, layers - at_z)):
                    if (way and at_z < layers - 1) or (not way and at_z > 0):
                        pieces = upb.at[pl.ds(0, reach * GROUP * depth), :]
                        wait_sent(pieces, piece_send.at[0, way])
                        wait_sent(downb.at[pl.ds(0, reach)], piece_send.at[1, way])

    drain_early()
    wait_sent(stage, part_send)

    @pl.when(mine_end)
    def _():
        lax.fori_loop(0, 2 * per_layer, finish, 0)

    wait_sent(peers, red_send)


def grouped(layers, tokens, norm_gain, up_weight, up_scale, down_weight, down_scale):
    rows, model = tokens.shape
    depth = up_weight.shape[0]
    if 2 * depth != COLS:
        return gathered(
            tokens, norm_gain, up_weight, up_scale, down_weight, down_scale
        )
    width = up_weight.shape[1] // GROUP
    share = model // COLS // CORES
    n = layers * GROUP
    dma = pltpu.SemaphoreType.DMA
    vmem = pl.BlockSpec(memory_space=pltpu.VMEM)
    hbm = pl.BlockSpec(memory_space=pltpu.HBM)
    ff = up_weight.shape[1]
    return pl.pallas_call(
        functools.partial(layer_kernel, layers, rows),
        out_shape=pltpu.VMEM((rows, model // CORES), jnp.bfloat16),
        in_specs=[hbm] * 6,
        out_specs=vmem,
        scratch_shapes=[
            pltpu.VMEM((1, model), jnp.float32),
            pltpu.VMEM((1, ff), jnp.float32),
            pltpu.VMEM((1, model), jnp.float32),
            pltpu.VMEM((GROUP * rows, model), jnp.bfloat16),
            pltpu.VMEM((model, width), jnp.bfloat16),
            pltpu.VMEM((layers, width, GROUP * depth), jnp.bfloat16),
            pltpu.VMEM((GROUP * rows, width), jnp.bfloat16),
            pltpu.VMEM((share, GROUP, 2, rows, COLS // 2), jnp.bfloat16),
            pltpu.VMEM((share, GROUP, 2, rows, COLS // 2), jnp.bfloat16),
            pltpu.VMEM((share, GROUP, 2, rows, COLS // 2), jnp.bfloat16),
            pltpu.VMEM((share, GROUP - 1, 2, rows, COLS // 2), jnp.bfloat16),
            pltpu.VMEM((GROUP, rows, COLS), jnp.float32),
            pltpu.VMEM((depth, GROUP * width), jnp.float32),
            pltpu.VMEM((GROUP * width, depth), jnp.float32),
            pltpu.VMEM((GROUP, depth, width), jnp.bfloat16),
            pltpu.VMEM((GROUP, width, depth), jnp.bfloat16),
            dma((7,)),
            dma((2, n)),
            dma((2, 2)),
            dma((2,)),
            dma((GROUP - 1, 2)),
            dma((GROUP - 1, 2)),
            dma((GROUP,)),
            dma((share, GROUP)),
            dma((share, 3)),
            dma((2, 2, 5)),
            dma((4,)),
        ],
        compiler_params=pltpu.CompilerParams(
            collective_id=0, has_side_effects=True, vmem_limit_bytes=60 * 2**20
        ),
    )(
        tokens, norm_gain.reshape(1, -1), up_weight, down_weight, up_scale.reshape(1, -1), down_scale
    )


def solution(mesh):
    fs, tp = mesh.shape["fs"], mesh.shape["tp"]
    if tp == CORES and fs % (2 * GROUP) == 0 and fs <= 4 * GROUP:
        body = functools.partial(grouped, fs // GROUP)
    else:
        body = gathered
    in_specs = (P("fs", None), P(), P("fs", "tp"), P("tp"), P("tp", "fs"), P())
    out_specs = P("fs", "tp")
    return jax.shard_map(
        body, mesh=mesh, in_specs=in_specs, out_specs=out_specs, check_vma=False
    )
```
